256 devices in a mesh: gr: 2 (over z_hi), sp: 16 (over z_lo, y), tp: 8 (over x, core).
Axes of the slice: x: 4, y: 4, z: 8 (z_hi: 2, z_lo: 4; z = z_hi * 4 + z_lo), core: 2. Of those that a mesh axis runs over, the one named last changes fastest.
Arguments:
- prompt: bfloat16 [256, 256, 1024], P('gr', 'sp'), parts along dimension 0, may hold values from -6 to 6
- w_key: bfloat16 [1024, 8, 128], P(None, 'tp'), may hold values from -0.1875 to 0.1875
- w_value: bfloat16 [1024, 8, 128], P(None, 'tp'), may hold values from -0.1875 to 0.1875
- w_in_gate: bfloat16 [2, 1024, 8], P(None, None, 'tp'), may hold values from -0.1875 to 0.1875
- w_forget_gate: bfloat16 [2, 1024, 8], P(None, None, 'tp'), may hold values from -0.1875 to 0.1875
- in_bias: float32 [2, 8], P(None, 'tp'), may hold values from -6 to 0, as said below
- forget_bias: float32 [2, 8], P(None, 'tp'), may hold values from 1 to 10, as said below
- query: bfloat16 [256, 8, 128], P(('gr', 'sp'), 'tp'), parts along dimension 0, may hold values from -6 to 6
- w_out: bfloat16 [8, 128, 1024], P('tp'), may hold values from -0.5 to 0.5
Outputs:
- memory: bfloat16 [2, 256, 8, 128, 128], P(None, ('gr', 'sp'), 'tp'), parts along dimension 1
- normalizer: float32 [2, 256, 8, 128], P(None, ('gr', 'sp'), 'tp'), parts along dimension 1
- stabilizer: float32 [2, 256, 8], P(None, ('gr', 'sp'), 'tp'), parts along dimension 1
- read: bfloat16 [256, 1024], P(('gr', 'sp'), 'tp'), parts along dimension 0
The draws below stay inside these ranges and needn't reach their ends.
There are 2 independent parts, one for each index of `gr`. The reference program is written for one: setup_inputs(seed, part) draws one part's arguments, and reference() takes and returns one part's arrays. A program takes and returns all parts, laid end to end along the dimension named above; an argument that names none is the same for every part. Nothing has to cross between parts.
Inputs may be any that keep to these rules, and one draw needn't show every extreme that they name: forget_bias lies between 1 and 10; the per-head share of memory kept over the whole prompt is spread between a few and some ninety percent. in_bias lies between -6 and 0.
All inputs are finite; a program needn't handle non-finite values.
Results may differ from the reference program's by a relative error of at most 0.015.
Values may be sent and summed in bfloat16 or wider, within the bound.
A program may use at most 64 MiB of HBM per device.

```python
import math
import jax
import jax.numpy as jnp
from jax import lax

D = 1024
HEADS = 8
HEAD_DIM = 128
SEQS = 128
SEQ_LEN = 256


def draw_forget_bias(key, part):
    kept_share = jnp.exp(jax.random.uniform(key, (2, HEADS), jnp.float32, math.log(0.05), math.log(0.9)))
    chain_loss = -jnp.log(kept_share) / 1.65
    return -jnp.log(jnp.expm1(chain_loss / SEQ_LEN))


def draw_in_bias(key, part):
    centre = -0.5 * math.log(SEQ_LEN) - 1.0
    offset = jax.random.uniform(key, (2, HEADS), jnp.float32, -1.0, 1.0)
    return offset + centre


def block_scale(stream_key, dims, shards, smallest, high):
    loudness, own = 1.0, jax.random.fold_in(stream_key, 6)
    for position, shards_of in shards:
        steps = jnp.exp(jax.random.uniform(jax.random.fold_in(own, position), (shards_of,), jnp.float32, smallest / len(shards), high / len(shards)))
        loudness = loudness * jnp.repeat(steps, dims[position] // shards_of).reshape([-1 if axis == position else 1 for axis in range(len(dims))])
    return loudness


def gaussian(key, extent, scale, reach, pieces=(), kind=jnp.bfloat16):
    loudness = block_scale(key, extent, pieces, -0.22, 0.18) if pieces else 1.0
    array = jax.random.normal(key, extent, jnp.float32) * scale * loudness
    return jnp.minimum(jnp.maximum(array, -reach), reach).astype(kind)


def setup_inputs(seed: int = 0, part: int = 0) -> dict:
    keys = jax.random.split(jax.random.key(seed), 10)
    part_keys = jax.random.split(jax.random.fold_in(keys[9], part), 10)
    prompt = gaussian(part_keys[0], (SEQS, SEQ_LEN, D), 1.0, 6.0, ((1, 16),))
    w_key = gaussian(keys[1], (D, HEADS, HEAD_DIM), D ** -0.5, 0.1875, ((1, 8),))
    w_value = gaussian(keys[2], (D, HEADS, HEAD_DIM), D ** -0.5, 0.1875, ((1, 8),))
    w_in_gate = gaussian(keys[3], (2, D, HEADS), D ** -0.5, 0.1875, ((2, 8),))
    w_forget_gate = gaussian(keys[4], (2, D, HEADS), D ** -0.5, 0.1875, ((2, 8),))
    in_bias = draw_in_bias(jax.random.fold_in(keys[9], 71), part)
    forget_bias = draw_forget_bias(jax.random.fold_in(keys[9], 71), part)
    query = gaussian(part_keys[7], (SEQS, HEADS, HEAD_DIM), 1.0, 6.0, ((0, 16), (1, 8)))
    w_out = gaussian(keys[8], (HEADS, HEAD_DIM, D), (HEADS * HEAD_DIM // 9) ** -0.5, 0.5, ((0, 8),))
    return dict(prompt=prompt, w_key=w_key, w_value=w_value, w_in_gate=w_in_gate, w_forget_gate=w_forget_gate, in_bias=in_bias, forget_bias=forget_bias, query=query, w_out=w_out)


highest = lax.Precision.HIGHEST


def summary(scaled, float_values, in_log, forget_log, backward):
    total_forget = jnp.sum(forget_log, axis=1)
    running = jnp.cumsum(forget_log, axis=1)
    if backward:
        log_weight = in_log + running - forget_log
    else:
        log_weight = in_log + total_forget[:, None, :] - running
    stable = jnp.maximum(total_forget, jnp.max(log_weight, axis=1))
    weight = jnp.exp(log_weight - stable[:, None, :])
    weighted = scaled * weight[..., None]
    memory = jnp.einsum('bshd,bshe->bhde', weighted, float_values, precision=highest)
    normal = jnp.sum(weighted, axis=1)
    return memory, normal, stable


def read_out(memory_bf, normal, stable, query_f):
    cells = memory_bf.astype(jnp.float32)
    numerator = jnp.sum(query_f[..., :, None] * cells, axis=-2)
    denominator = jnp.sum(query_f * normal, axis=-1)
    floor_value = jnp.maximum(jnp.maximum(jnp.abs(denominator), jnp.exp(-stable)), 1.0)
    return numerator / floor_value[..., None]


def reference(prompt, w_key, w_value, w_in_gate, w_forget_gate, in_bias, forget_bias, query, w_out):
    token_rows = prompt.astype(jnp.float32)
    key_rows = jnp.einsum('bsd,dhe->bshe', token_rows, w_key.astype(jnp.float32), precision=highest).astype(jnp.bfloat16)
    value_rows = jnp.einsum('bsd,dhe->bshe', token_rows, w_value.astype(jnp.float32), precision=highest).astype(jnp.bfloat16)
    in_pre = jnp.einsum('bsd,gdh->bsgh', token_rows, w_in_gate.astype(jnp.float32), precision=highest) + in_bias
    forget_pre = jnp.einsum('bsd,gdh->bsgh', token_rows, w_forget_gate.astype(jnp.float32), precision=highest) + forget_bias
    scaled = key_rows.astype(jnp.float32) * (key_rows.shape[-1] ** -0.5)
    float_values = value_rows.astype(jnp.float32)
    query_f = query.astype(jnp.float32)
    memories = []
    normals = []
    stables = []
    reads = []
    for course in range(2):
        memory, normal, stable = summary(scaled, float_values, in_pre[:, :, course, :],
                                         jax.nn.log_sigmoid(forget_pre[:, :, course, :]), course == 1)
        memory_bf = memory.astype(jnp.bfloat16)
        memories.append(memory_bf)
        normals.append(normal)
        stables.append(stable)
        reads.append(read_out(memory_bf, normal, stable, query_f))
    hidden = (reads[0] + reads[1]).astype(jnp.bfloat16)
    read = jnp.einsum('bhd,hde->be', hidden.astype(jnp.float32), w_out.astype(jnp.float32), precision=highest).astype(jnp.bfloat16)
    return (jnp.stack(memories), jnp.stack(normals), jnp.stack(stables), read)
```

```python
import functools

import jax
import jax.numpy as jnp
from jax import lax
from jax.experimental import pallas as pl
from jax.experimental.pallas import tpu as pltpu
from jax.sharding import Mesh
from jax.sharding import PartitionSpec as P

MESH = pl.DeviceIdType.MESH
TP = ("x", "c")
F32 = jnp.float32
BF16 = jnp.bfloat16
FAR = 12


def offsets(k):
    return lax.rem(k, 3) + 1, k // 3


def kernel(
    prompt, w_key, w_value, w_gate, in_bias, forget_bias, query, w_out,
    memory_out, normal_out, stable_out, read_out,
    rows, weights, gate_w, out_w, keys, values, gates, terms, parts,
    load_sem, far_send, far_recv, near_send, near_recv, x_send, x_recv, swap_send, swap_recv, term_send, term_recv,
):
    z, y, x, c = (lax.axis_index(a) for a in ("z", "y", "x", "c"))
    here = z * 4 + y
    seq = 4 * c + x
    up = lax.rem(x + 1 + 2 * c, 4)
    down = lax.rem(x + 3 + 2 * c, 4)
    across = lax.rem(x + 2, 4)

    loads = [
        pltpu.make_async_copy(w_key, weights.at[:, pl.ds(0, 128)], load_sem.at[0]),
        pltpu.make_async_copy(w_value, weights.at[:, pl.ds(128, 128)], load_sem.at[1]),
        pltpu.make_async_copy(prompt.at[pl.ds(here * 8, 8)], rows.at[here], load_sem.at[2]),
        pltpu.make_async_copy(w_out, out_w, load_sem.at[3]),
    ]
    for load in loads:
        load.start()

    barrier = pltpu.get_barrier_semaphore()

    @pl.loop(1, 16)
    def _(k):
        to = {"z": lax.rem(z + k // 4, 4), "y": lax.rem(y + lax.rem(k, 4), 4)}
        pl.semaphore_signal(barrier, inc=1, device_id=to, device_id_type=MESH)

    @pl.loop(1, 8)
    def _(k):
        to = {"x": lax.rem(x + k // 2, 4), "c": lax.rem(c + lax.rem(k, 2), 2)}
        pl.semaphore_signal(barrier, inc=1, device_id=to, device_id_type=MESH)

    pl.semaphore_wait(barrier, 22)

    def far(k):
        dz, dy = offsets(k)
        tz, ty = lax.rem(z + dz, 4), lax.rem(y + dy, 4)
        return pltpu.make_async_remote_copy(
            src_ref=prompt.at[(tz * 4 + ty) * 8 + seq],
            dst_ref=rows.at[here, seq],
            send_sem=far_send.at[k],
            recv_sem=far_recv.at[k],
            device_id={"z": tz, "y": ty},
            device_id_type=MESH,
        )

    def near(k):
        ty = lax.rem(y + k + 1, 4)
        return pltpu.make_async_remote_copy(
            src_ref=prompt.at[pl.ds((z * 4 + ty) * 8 + 4 * c, 4)],
            dst_ref=rows.at[here, pl.ds(4 * c, 4)],
            send_sem=near_send.at[k],
            recv_sem=near_recv.at[k],
            device_id={"y": ty},
            device_id_type=MESH,
        )

    def source(k):
        dz, dy = offsets(k)
        return lax.rem(z + 4 - dz, 4) * 4 + lax.rem(y + 4 - dy, 4)

    def near_source(k):
        return z * 4 + lax.rem(y + 3 - k, 4)

    def along_x(k, which):
        held = seq if which < 2 else 4 * c + down
        block = rows.at[source(k), held]
        return pltpu.make_async_remote_copy(
            src_ref=block,
            dst_ref=block,
            send_sem=x_send.at[k, which],
            recv_sem=x_recv.at[k, which],
            device_id={"x": down if which == 1 else up},
            device_id_type=MESH,
        )

    def swap(k, src):
        block = rows.at[src, pl.ds(4 * c, 4)]
        return pltpu.make_async_remote_copy(
            src_ref=block,
            dst_ref=block,
            send_sem=swap_send.at[k],
            recv_sem=swap_recv.at[k],
            device_id={"c": 1 - c},
            device_id_type=MESH,
        )

    @pl.loop(0, FAR)
    def _(k):
        far(k).start()

    @pl.loop(0, 3)
    def _(k):
        near(k).start()

    lane8 = lax.broadcasted_iota(jnp.int32, (8, 128), 1) // 8
    gate8 = lax.broadcasted_iota(jnp.int32, (8, 128), 0)
    spread = jnp.where(lane8 == gate8, 1.0, 0.0).astype(BF16)
    gate_w[...] = lax.dot_general(
        w_gate[...], spread, (((0,), (0,)), ((), ())), preferred_element_type=F32
    ).astype(BF16)

    lane = lax.broadcasted_iota(jnp.int32, (8, 16, 128), 2)
    which_seq = lax.broadcasted_iota(jnp.int32, (8, 16, 128), 0)
    own_lane = lax.rem(lane, 8) == which_seq

    def project(src):
        block = rows[src].reshape(128, 1024)
        both = jnp.dot(block, weights[...], preferred_element_type=F32)
        at = pl.ds(pl.multiple_of(src * 16, 16), 16)
        keys[:, at, :] = both[:, :128].astype(BF16).reshape(8, 16, 128)
        values[:, at, :] = both[:, 128:].astype(BF16).reshape(8, 16, 128)
        pre = jnp.dot(block, gate_w[...], preferred_element_type=F32).reshape(8, 16, 128)
        gates[at, :] = jnp.sum(jnp.where(own_lane, pre, 0.0), axis=0)

    for load in loads:
        load.wait()
    project(here)

    @pl.loop(0, FAR + 3)
    def _(step):
        @pl.when(step < FAR)
        def _():
            far(step).wait_recv()
            along_x(step, 0).start()
            along_x(step, 1).start()

        @pl.when((step >= 1) & (step < FAR + 1))
        def _():
            along_x(step - 1, 0).wait_recv()
            along_x(step - 1, 2).start()

        @pl.when((step >= 2) & (step < FAR + 2))
        def _():
            along_x(step - 2, 1).wait_recv()
            along_x(step - 2, 2).wait_recv()
            swap(step - 2, source(step - 2)).start()

        @pl.when((step >= 6) & (step < 9))
        def _():
            near(step - 6).wait_recv()
            swap(FAR + step - 6, near_source(step - 6)).start()

        @pl.when(step >= 3)
        def _():
            swap(step - 3, source(step - 3)).wait_recv()
            project(source(step - 3))

        @pl.when((step >= 8) & (step < 11))
        def _():
            swap(FAR + step - 8, near_source(step - 8)).wait_recv()
            project(near_source(step - 8))

    lane1 = lax.broadcasted_iota(jnp.int32, (1, 128), 1)
    bias = jnp.where(
        lane1 < 16,
        jnp.where(lane1 < 8, in_bias[0, 0], in_bias[1, 0]),
        jnp.where(lane1 < 24, forget_bias[0, 0], forget_bias[1, 0]),
    )
    pre = gates[...] + bias
    forget = pltpu.roll(jax.nn.log_sigmoid(pre), 112, 1)
    row = lax.broadcasted_iota(jnp.int32, (256, 256), 0)
    col = lax.broadcasted_iota(jnp.int32, (256, 256), 1)
    lower = jnp.where(col < row, 1.0, 0.0)
    before = jnp.dot(lower, forget, preferred_element_type=F32, precision=lax.Precision.HIGHEST)
    total = before[255:256, :] + forget[255:256, :]
    log_weight = pre + jnp.where(lane1 < 8, total - before - forget, before)
    stable = jnp.maximum(total, jnp.max(log_weight, axis=0, keepdims=True))
    weight = jnp.exp(log_weight - stable) * 128.0**-0.5
    stable_out[0:1, :] = stable[:, 0:8]
    stable_out[1:2, :] = pltpu.roll(stable, 120, 1)[:, 0:8]

    query_rows = query[...]
    numerators = []
    normals = ([], [])
    for b in range(8):
        float_keys = keys[b].astype(F32)
        float_values = values[b].astype(F32)
        weighted = []
        for g in range(2):
            spread_weight = jnp.broadcast_to(weight[:, 8 * g + b : 8 * g + b + 1], (256, 128))
            weighted.append((float_values * spread_weight).astype(BF16))
            normals[g].append(jnp.sum(float_keys * spread_weight, axis=0, keepdims=True))
        cells = lax.dot_general(
            keys[b], jnp.concatenate(weighted, axis=1), (((0,), (0,)), ((), ())), preferred_element_type=F32
        ).astype(BF16)
        memory_out[0, b] = cells[:, :128]
        memory_out[1, b] = cells[:, 128:]
        numerators.append(jnp.dot(query_rows, cells, preferred_element_type=F32)[b : b + 1])
    numerator = jnp.concatenate(numerators, axis=0)

    seq8 = lax.broadcasted_iota(jnp.int32, (8, 128), 0)
    lane8 = lax.broadcasted_iota(jnp.int32, (8, 128), 1)
    float_query = query_rows.astype(F32)
    hidden = jnp.zeros((8, 128), F32)
    for g in range(2):
        normal = jnp.concatenate(normals[g], axis=0)
        normal_out[g] = normal
        denominator = jnp.sum(float_query * normal, axis=1, keepdims=True)
        own_stable = jnp.sum(
            jnp.where(lane8 == 8 * g + seq8, jnp.broadcast_to(stable, (8, 128)), 0.0), axis=1, keepdims=True
        )
        floor_value = jnp.maximum(jnp.maximum(jnp.abs(denominator), jnp.exp(-own_stable)), 1.0)
        hidden = hidden + numerator[:, 128 * g : 128 * g + 128] / floor_value
    head_terms = jnp.dot(hidden.astype(BF16), out_w[...], preferred_element_type=F32)
    for t in range(8):
        terms[t] = head_terms[:, 128 * t : 128 * t + 128]

    me = 2 * x + c

    def term(k):
        tx, tc = lax.rem(x + k // 2, 4), lax.rem(c + lax.rem(k, 2), 2)
        return pltpu.make_async_remote_copy(
            src_ref=terms.at[2 * tx + tc],
            dst_ref=parts.at[k],
            send_sem=term_send.at[k],
            recv_sem=term_recv.at[k],
            device_id={"x": tx, "c": tc},
            device_id_type=MESH,
        )

    @pl.loop(1, 8)
    def _(k):
        term(k).start()

    @pl.loop(0, FAR)
    def _(k):
        far(k).wait_send()
        swap(k, source(k)).wait_send()
        for which in range(3):
            along_x(k, which).wait_send()

    @pl.loop(0, 3)
    def _(k):
        near(k).wait_send()
        swap(FAR + k, near_source(k)).wait_send()

    @pl.loop(1, 8)
    def _(k):
        term(k).wait_recv()

    total_read = terms[me]
    for k in range(1, 8):
        total_read = total_read + parts[k]
    read_out[...] = total_read.astype(BF16)

    @pl.loop(1, 8)
    def _(k):
        term(k).wait_send()


def shards(prompt, w_key, w_value, w_in_gate, w_forget_gate, in_bias, forget_bias, query, w_out):
    w_gate = jnp.concatenate(
        [w_in_gate[:, :, 0], w_forget_gate[:, :, 0], jnp.zeros((4, 1024), BF16)], axis=0
    )
    vmem = pl.BlockSpec(memory_space=pltpu.VMEM)
    smem = pl.BlockSpec(memory_space=pltpu.SMEM)
    anywhere = pl.BlockSpec(memory_space=pl.ANY)
    dma = pltpu.SemaphoreType.DMA
    memory, normal, stable, read = pl.pallas_call(
        kernel,
        out_shape=(
            jax.ShapeDtypeStruct((2, 8, 128, 128), BF16),
            jax.ShapeDtypeStruct((2, 8, 128), F32),
            jax.ShapeDtypeStruct((2, 8), F32),
            jax.ShapeDtypeStruct((8, 128), BF16),
        ),
        in_specs=[anywhere, anywhere, anywhere, vmem, smem, smem, vmem, anywhere],
        out_specs=(vmem, vmem, vmem, vmem),
        scratch_shapes=[
            pltpu.VMEM((16, 8, 16, 1024), BF16),
            pltpu.VMEM((1024, 256), BF16),
            pltpu.VMEM((1024, 128), BF16),
            pltpu.VMEM((128, 1024), BF16),
            pltpu.VMEM((8, 256, 128), BF16),
            pltpu.VMEM((8, 256, 128), BF16),
            pltpu.VMEM((256, 128), F32),
            pltpu.VMEM((8, 8, 128), F32),
            pltpu.VMEM((8, 8, 128), F32),
            dma((4,)),
            dma((FAR,)),
            dma((FAR,)),
            dma((3,)),
            dma((3,)),
            dma((FAR, 3)),
            dma((FAR, 3)),
            dma((FAR + 3,)),
            dma((FAR + 3,)),
            dma((8,)),
            dma((8,)),
        ],
        compiler_params=pltpu.CompilerParams(
            collective_id=0, has_side_effects=True, vmem_limit_bytes=32 * 1024 * 1024
        ),
    )(
        prompt, w_key[:, 0], w_value[:, 0], w_gate, in_bias, forget_bias, query[:, 0], w_out[0]
    )
    return memory[:, :, None], normal[:, :, None], stable[:, :, None], read


def solution(mesh):
    torus = Mesh(
        mesh.devices.reshape(mesh.shape["gr"], 4, 4, 4, 2), ("gr", "z", "y", "x", "c")
    )
    sp = ("z", "y")
    both = ("gr", "z", "y")
    return jax.shard_map(
        shards,
        mesh=torus,
        in_specs=(
            P("gr", sp, None),
            P(None, TP, None),
            P(None, TP, None),
            P(None, None, TP),
            P(None, None, TP),
            P(None, TP),
            P(None, TP),
            P(both, TP, None),
            P(TP, None, None),
        ),
        out_specs=(
            P(None, both, TP, None, None),
            P(None, both, TP, None),
            P(None, both, TP),
            P(both, TP),
        ),
        check_vma=False,
    )
```

```python
import functools

import jax
import jax.numpy as jnp
from jax import lax
from jax.experimental import pallas as pl
from jax.experimental.pallas import tpu as pltpu
from jax.sharding import Mesh
from jax.sharding import PartitionSpec as P

MESH = pl.DeviceIdType.MESH
TP = ("x", "c")
F32 = jnp.float32
BF16 = jnp.bfloat16
FAR = 12


def offsets(k):
    return lax.rem(k, 3) + 1, k // 3


def kernel(
    prompt, w_key, w_value, w_in, w_forget, in_bias, forget_bias, query, w_out,
    memory_out, normal_out, stable_out, read_out,
    rows, weights, gate_rows, gate_w, biases, queries, out_w, keys, values, gates, terms, parts,
    load_sem, far_send, far_recv, near_send, near_recv, x_send, x_recv, swap_send, swap_recv, term_send, term_recv,
):
    z, y, x, c = (lax.axis_index(a) for a in ("z", "y", "x", "c"))
    here = z * 4 + y
    seq = 4 * c + x
    up = lax.rem(x + 1 + 2 * c, 4)
    down = lax.rem(x + 3 + 2 * c, 4)
    across = lax.rem(x + 2, 4)

    loads = [
        pltpu.make_async_copy(w_key, weights.at[:, pl.ds(0, 128)], load_sem.at[0]),
        pltpu.make_async_copy(w_value, weights.at[:, pl.ds(128, 128)], load_sem.at[1]),
        pltpu.make_async_copy(prompt.at[pl.ds(here * 8, 8)], rows.at[here], load_sem.at[2]),
        pltpu.make_async_copy(w_in, gate_rows.at[0], load_sem.at[3]),
        pltpu.make_async_copy(w_forget, gate_rows.at[1], load_sem.at[4]),
        pltpu.make_async_copy(in_bias, biases.at[pl.ds(0, 1)], load_sem.at[5]),
        pltpu.make_async_copy(forget_bias, biases.at[pl.ds(1, 1)], load_sem.at[6]),
        pltpu.make_async_copy(query, queries, load_sem.at[7]),
        pltpu.make_async_copy(w_out, out_w, load_sem.at[8]),
    ]
    for load in loads:
        load.start()

    barrier = pltpu.get_barrier_semaphore()

    @pl.loop(1, 16)
    def _(k):
        to = {"z": lax.rem(z + k // 4, 4), "y": lax.rem(y + lax.rem(k, 4), 4)}
        pl.semaphore_signal(barrier, inc=1, device_id=to, device_id_type=MESH)

    @pl.loop(1, 8)
    def _(k):
        to = {"x": lax.rem(x + k // 2, 4), "c": lax.rem(c + lax.rem(k, 2), 2)}
        pl.semaphore_signal(barrier, inc=1, device_id=to, device_id_type=MESH)

    pl.semaphore_wait(barrier, 22)

    def far(k):
        dz, dy = offsets(k)
        tz, ty = lax.rem(z + dz, 4), lax.rem(y + dy, 4)
        return pltpu.make_async_remote_copy(
            src_ref=prompt.at[(tz * 4 + ty) * 8 + seq],
            dst_ref=rows.at[here, seq],
            send_sem=far_send.at[k],
            recv_sem=far_recv.at[k],
            device_id={"z": tz, "y": ty},
            device_id_type=MESH,
        )

    def near(k):
        ty = lax.rem(y + k + 1, 4)
        return pltpu.make_async_remote_copy(
            src_ref=prompt.at[pl.ds((z * 4 + ty) * 8 + 4 * c, 4)],
            dst_ref=rows.at[here, pl.ds(4 * c, 4)],
            send_sem=near_send.at[k],
            recv_sem=near_recv.at[k],
            device_id={"y": ty},
            device_id_type=MESH,
        )

    def source(k):
        dz, dy = offsets(k)
        return lax.rem(z + 4 - dz, 4) * 4 + lax.rem(y + 4 - dy, 4)

    def near_source(k):
        return z * 4 + lax.rem(y + 3 - k, 4)

    def along_x(k, which):
        held = seq if which < 2 else 4 * c + down
        block = rows.at[source(k), held]
        return pltpu.make_async_remote_copy(
            src_ref=block,
            dst_ref=block,
            send_sem=x_send.at[k, which],
            recv_sem=x_recv.at[k, which],
            device_id={"x": down if which == 1 else up},
            device_id_type=MESH,
        )

    def swap(k, src):
        block = rows.at[src, pl.ds(4 * c, 4)]
        return pltpu.make_async_remote_copy(
            src_ref=block,
            dst_ref=block,
            send_sem=swap_send.at[k],
            recv_sem=swap_recv.at[k],
            device_id={"c": 1 - c},
            device_id_type=MESH,
        )

    @pl.loop(0, FAR)
    def _(k):
        far(k).start()

    @pl.loop(0, 3)
    def _(k):
        near(k).start()

    for load in loads:
        load.wait()

    lane_gate = lax.broadcasted_iota(jnp.int32, (2, 128), 1) // 8
    gate2 = lax.broadcasted_iota(jnp.int32, (2, 128), 0)
    spread_gates = 0.0
    for kind in range(2):
        spread = jnp.where(lane_gate == 2 * kind + gate2, 1.0, 0.0).astype(BF16)
        spread_gates = spread_gates + lax.dot_general(
            gate_rows[kind], spread, (((0,), (0,)), ((), ())), preferred_element_type=F32
        )
    gate_w[...] = spread_gates.astype(BF16)

    lane = lax.broadcasted_iota(jnp.int32, (8, 16, 128), 2)
    which_seq = lax.broadcasted_iota(jnp.int32, (8, 16, 128), 0)
    own_lane = lax.rem(lane, 8) == which_seq

    def project(src):
        block = rows[src].reshape(128, 1024)
        both = jnp.dot(block, weights[...], preferred_element_type=F32)
        at = pl.ds(pl.multiple_of(src * 16, 16), 16)
        keys[:, at, :] = both[:, :128].astype(BF16).reshape(8, 16, 128)
        values[:, at, :] = both[:, 128:].astype(BF16).reshape(8, 16, 128)
        pre = jnp.dot(block, gate_w[...], preferred_element_type=F32).reshape(8, 16, 128)
        gates[at, :] = jnp.sum(jnp.where(own_lane, pre, 0.0), axis=0)

    project(here)

    @pl.loop(0, FAR + 3)
    def _(step):
        @pl.when(step < FAR)
        def _():
            far(step).wait_recv()
            along_x(step, 0).start()
            along_x(step, 1).start()

        @pl.when((step >= 1) & (step < FAR + 1))
        def _():
            along_x(step - 1, 0).wait_recv()
            along_x(step - 1, 2).start()

        @pl.when((step >= 2) & (step < FAR + 2))
        def _():
            along_x(step - 2, 1).wait_recv()
            along_x(step - 2, 2).wait_recv()
            swap(step - 2, source(step - 2)).start()

        @pl.when((step >= 6) & (step < 9))
        def _():
            near(step - 6).wait_recv()
            swap(FAR + step - 6, near_source(step - 6)).start()

        @pl.when(step >= 3)
        def _():
            swap(step - 3, source(step - 3)).wait_recv()
            project(source(step - 3))

        @pl.when((step >= 8) & (step < 11))
        def _():
            swap(FAR + step - 8, near_source(step - 8)).wait_recv()
            project(near_source(step - 8))

    lane1 = lax.broadcasted_iota(jnp.int32, (1, 128), 1)
    bias = jnp.where(
        lane1 < 16,
        jnp.where(lane1 < 8, biases[0:1, 0:1], biases[0:1, 1:2]),
        jnp.where(lane1 < 24, biases[1:2, 0:1], biases[1:2, 1:2]),
    )
    pre = gates[...] + bias
    forget = pltpu.roll(jax.nn.log_sigmoid(pre), 112, 1)
    row = lax.broadcasted_iota(jnp.int32, (256, 256), 0)
    col = lax.broadcasted_iota(jnp.int32, (256, 256), 1)
    lower = jnp.where(col < row, 1.0, 0.0)
    before = jnp.dot(lower, forget, preferred_element_type=F32, precision=lax.Precision.HIGHEST)
    total = before[255:256, :] + forget[255:256, :]
    log_weight = pre + jnp.where(lane1 < 8, total - before - forget, before)
    stable = jnp.maximum(total, jnp.max(log_weight, axis=0, keepdims=True))
    weight = jnp.exp(log_weight - stable) * 128.0**-0.5
    stable_out[0:1, :] = stable[:, 0:8]
    stable_out[1:2, :] = pltpu.roll(stable, 120, 1)[:, 0:8]

    query_rows = queries[...]
    numerators = []
    normals = ([], [])
    for b in range(8):
        float_keys = keys[b].astype(F32)
        float_values = values[b].astype(F32)
        weighted = []
        for g in range(2):
            spread_weight = jnp.broadcast_to(weight[:, 8 * g + b : 8 * g + b + 1], (256, 128))
            weighted.append((float_values * spread_weight).astype(BF16))
            normals[g].append(jnp.sum(float_keys * spread_weight, axis=0, keepdims=True))
        cells = lax.dot_general(
            keys[b], jnp.concatenate(weighted, axis=1), (((0,), (0,)), ((), ())), preferred_element_type=F32
        ).astype(BF16)
        memory_out[0, b] = cells[:, :128]
        memory_out[1, b] = cells[:, 128:]
        numerators.append(jnp.dot(query_rows, cells, preferred_element_type=F32)[b : b + 1])
    numerator = jnp.concatenate(numerators, axis=0)

    seq8 = lax.broadcasted_iota(jnp.int32, (8, 128), 0)
    lane8 = lax.broadcasted_iota(jnp.int32, (8, 128), 1)
    float_query = query_rows.astype(F32)
    hidden = jnp.zeros((8, 128), F32)
    for g in range(2):
        normal = jnp.concatenate(normals[g], axis=0)
        normal_out[g] = normal
        denominator = jnp.sum(float_query * normal, axis=1, keepdims=True)
        own_stable = jnp.sum(
            jnp.where(lane8 == 8 * g + seq8, jnp.broadcast_to(stable, (8, 128)), 0.0), axis=1, keepdims=True
        )
        floor_value = jnp.maximum(jnp.maximum(jnp.abs(denominator), jnp.exp(-own_stable)), 1.0)
        hidden = hidden + numerator[:, 128 * g : 128 * g + 128] / floor_value
    head_terms = jnp.dot(hidden.astype(BF16), out_w[...], preferred_element_type=F32)
    for t in range(8):
        terms[t] = head_terms[:, 128 * t : 128 * t + 128]

    me = 2 * x + c

    def term(k):
        tx, tc = lax.rem(x + k // 2, 4), lax.rem(c + lax.rem(k, 2), 2)
        return pltpu.make_async_remote_copy(
            src_ref=terms.at[2 * tx + tc],
            dst_ref=parts.at[k],
            send_sem=term_send.at[k],
            recv_sem=term_recv.at[k],
            device_id={"x": tx, "c": tc},
            device_id_type=MESH,
        )

    @pl.loop(1, 8)
    def _(k):
        term(k).start()

    @pl.loop(0, FAR)
    def _(k):
        far(k).wait_send()
        swap(k, source(k)).wait_send()
        for which in range(3):
            along_x(k, which).wait_send()

    @pl.loop(0, 3)
    def _(k):
        near(k).wait_send()
        swap(FAR + k, near_source(k)).wait_send()

    @pl.loop(1, 8)
    def _(k):
        term(k).wait_recv()

    total_read = terms[me]
    for k in range(1, 8):
        total_read = total_read + parts[k]
    read_out[...] = total_read.astype(BF16)

    @pl.loop(1, 8)
    def _(k):
        term(k).wait_send()


def shards(prompt, w_key, w_value, w_in_gate, w_forget_gate, in_bias, forget_bias, query, w_out):
    vmem = pl.BlockSpec(memory_space=pltpu.VMEM)
    hbm = pl.BlockSpec(memory_space=pltpu.HBM)
    dma = pltpu.SemaphoreType.DMA
    memory, normal, stable, read = pl.pallas_call(
        kernel,
        out_shape=(
            jax.ShapeDtypeStruct((2, 8, 128, 128), BF16),
            jax.ShapeDtypeStruct((2, 8, 128), F32),
            jax.ShapeDtypeStruct((2, 8), F32),
            jax.ShapeDtypeStruct((8, 128), BF16),
        ),
        in_specs=[hbm] * 9,
        out_specs=(vmem, vmem, vmem, vmem),
        scratch_shapes=[
            pltpu.VMEM((16, 8, 16, 1024), BF16),
            pltpu.VMEM((1024, 256), BF16),
            pltpu.VMEM((2, 2, 1024), BF16),
            pltpu.VMEM((1024, 128), BF16),
            pltpu.VMEM((2, 2), F32),
            pltpu.VMEM((8, 128), BF16),
            pltpu.VMEM((128, 1024), BF16),
            pltpu.VMEM((8, 256, 128), BF16),
            pltpu.VMEM((8, 256, 128), BF16),
            pltpu.VMEM((256, 128), F32),
            pltpu.VMEM((8, 8, 128), F32),
            pltpu.VMEM((8, 8, 128), F32),
            dma((9,)),
            dma((FAR,)),
            dma((FAR,)),
            dma((3,)),
            dma((3,)),
            dma((FAR, 3)),
            dma((FAR, 3)),
            dma((FAR + 3,)),
            dma((FAR + 3,)),
            dma((8,)),
            dma((8,)),
        ],
        compiler_params=pltpu.CompilerParams(
            collective_id=0, has_side_effects=True, vmem_limit_bytes=60 * 1024 * 1024
        ),
    )(
        prompt, w_key[:, 0], w_value[:, 0], w_in_gate[:, :, 0], w_forget_gate[:, :, 0],
        in_bias.T, forget_bias.T, query[:, 0], w_out[0],
    )
    return memory[:, :, None], normal[:, :, None], stable[:, :, None], read


def solution(mesh):
    torus = Mesh(
        mesh.devices.reshape(mesh.shape["gr"], 4, 4, 4, 2), ("gr", "z", "y", "x", "c")
    )
    sp = ("z", "y")
    both = ("gr", "z", "y")
    return jax.shard_map(
        shards,
        mesh=torus,
        in_specs=(
            P("gr", sp, None),
            P(None, TP, None),
            P(None, TP, None),
            P(None, None, TP),
            P(None, None, TP),
            P(None, TP),
            P(None, TP),
            P(both, TP, None),
            P(TP, None, None),
        ),
        out_specs=(
            P(None, both, TP, None, None),
            P(None, both, TP, None),
            P(None, both, TP),
            P(both, TP),
        ),
        check_vma=False,
    )
```

```python
import functools

import jax
import jax.numpy as jnp
from jax import lax
from jax.experimental import pallas as pl
from jax.experimental.pallas import tpu as pltpu
from jax.sharding import Mesh
from jax.sharding import PartitionSpec as P

MESH = pl.DeviceIdType.MESH
TP = ("x", "c")
F32 = jnp.float32
BF16 = jnp.bfloat16
FAR = 12


def offsets(k):
    return lax.rem(k, 3) + 1, k // 3


def kernel(
    prompt, w_key, w_value, w_in, w_forget, in_bias, forget_bias, query, w_out,
    memory_out, normal_out, stable_out, read_out,
    rows, weights, gate_rows, gate_w, biases, queries, query_w, out_w, keys, values, gates, scores, terms, parts,
    load_sem, far_send, far_recv, near_send, near_recv, x_send, x_recv, swap_send, swap_recv, term_send, term_recv,
):
    z, y, x, c = (lax.axis_index(a) for a in ("z", "y", "x", "c"))
    here = z * 4 + y
    seq = 4 * c + x
    up = lax.rem(x + 1 + 2 * c, 4)
    down = lax.rem(x + 3 + 2 * c, 4)
    across = lax.rem(x + 2, 4)

    loads = [
        pltpu.make_async_copy(w_key, weights.at[:, pl.ds(0, 128)], load_sem.at[0]),
        pltpu.make_async_copy(w_value, weights.at[:, pl.ds(128, 128)], load_sem.at[1]),
        pltpu.make_async_copy(prompt.at[pl.ds(here * 8, 8)], rows.at[here], load_sem.at[2]),
        pltpu.make_async_copy(w_in, gate_rows.at[0], load_sem.at[3]),
        pltpu.make_async_copy(w_forget, gate_rows.at[1], load_sem.at[4]),
        pltpu.make_async_copy(in_bias, biases.at[pl.ds(0, 1)], load_sem.at[5]),
        pltpu.make_async_copy(forget_bias, biases.at[pl.ds(1, 1)], load_sem.at[6]),
        pltpu.make_async_copy(query, queries, load_sem.at[7]),
        pltpu.make_async_copy(w_out, out_w, load_sem.at[8]),
    ]
    for load in loads:
        load.start()

    barrier = pltpu.get_barrier_semaphore()

    @pl.loop(1, 16)
    def _(k):
        to = {"z": lax.rem(z + k // 4, 4), "y": lax.rem(y + lax.rem(k, 4), 4)}
        pl.semaphore_signal(barrier, inc=1, device_id=to, device_id_type=MESH)

    @pl.loop(1, 8)
    def _(k):
        to = {"x": lax.rem(x + k // 2, 4), "c": lax.rem(c + lax.rem(k, 2), 2)}
        pl.semaphore_signal(barrier, inc=1, device_id=to, device_id_type=MESH)

    pl.semaphore_wait(barrier, 22)

    def far(k):
        dz, dy = offsets(k)
        tz, ty = lax.rem(z + dz, 4), lax.rem(y + dy, 4)
        return pltpu.make_async_remote_copy(
            src_ref=prompt.at[(tz * 4 + ty) * 8 + seq],
            dst_ref=rows.at[here, seq],
            send_sem=far_send.at[k],
            recv_sem=far_recv.at[k],
            device_id={"z": tz, "y": ty},
            device_id_type=MESH,
        )

    def near_offset(k):
        return lax.rem(2 * k + 1 - k // 2 * 3, 4)

    def near(k):
        ty = lax.rem(y + near_offset(k), 4)
        return pltpu.make_async_remote_copy(
            src_ref=prompt.at[pl.ds((z * 4 + ty) * 8 + 4 * c, 4)],
            dst_ref=rows.at[here, pl.ds(4 * c, 4)],
            send_sem=near_send.at[k],
            recv_sem=near_recv.at[k],
            device_id={"y": ty},
            device_id_type=MESH,
        )

    def source(k):
        dz, dy = offsets(k)
        return lax.rem(z + 4 - dz, 4) * 4 + lax.rem(y + 4 - dy, 4)

    def near_source(k):
        return z * 4 + lax.rem(y + 4 - near_offset(k), 4)

    def along_x(k, which):
        held = seq if which < 2 else 4 * c + down
        block = rows.at[source(k), held]
        return pltpu.make_async_remote_copy(
            src_ref=block,
            dst_ref=block,
            send_sem=x_send.at[k, which],
            recv_sem=x_recv.at[k, which],
            device_id={"x": down if which == 1 else up},
            device_id_type=MESH,
        )

    def swap(k, src):
        block = rows.at[src, pl.ds(4 * c, 4)]
        return pltpu.make_async_remote_copy(
            src_ref=block,
            dst_ref=block,
            send_sem=swap_send.at[k],
            recv_sem=swap_recv.at[k],
            device_id={"c": 1 - c},
            device_id_type=MESH,
        )

    @pl.loop(0, 12)
    def _(k):
        far(k).start()

    near(0).start()
    near(1).start()
    near(2).start()

    for load in loads:
        load.wait()

    lane_gate = lax.broadcasted_iota(jnp.int32, (2, 128), 1) // 8
    gate2 = lax.broadcasted_iota(jnp.int32, (2, 128), 0)
    spread_gates = 0.0
    for kind in range(2):
        spread = jnp.where(lane_gate == 2 * kind + gate2, 1.0, 0.0).astype(BF16)
        spread_gates = spread_gates + lax.dot_general(
            gate_rows[kind], spread, (((0,), (0,)), ((), ())), preferred_element_type=F32
        )
    gate_w[...] = spread_gates.astype(BF16)

    lane8 = lax.broadcasted_iota(jnp.int32, (8, 128), 1)
    pick = jnp.where(lax.rem(lane8, 8) == lax.broadcasted_iota(jnp.int32, (8, 128), 0), 1.0, 0.0)
    query_w[...] = lax.dot_general(
        queries[...], pick.astype(BF16), (((0,), (0,)), ((), ())), preferred_element_type=F32
    ).astype(BF16)

    lane = lax.broadcasted_iota(jnp.int32, (8, 16, 128), 2)
    which_seq = lax.broadcasted_iota(jnp.int32, (8, 16, 128), 0)
    own_lane = lax.rem(lane, 8) == which_seq

    def project(src):
        block = rows[src].reshape(128, 1024)
        both = jnp.dot(block, weights[...], preferred_element_type=F32)
        at = pl.ds(pl.multiple_of(src * 16, 16), 16)
        key_rows = both[:, :128].astype(BF16)
        keys[:, at, :] = key_rows.reshape(8, 16, 128)
        values[:, at, :] = both[:, 128:].astype(BF16).reshape(8, 16, 128)
        pre = jnp.dot(block, gate_w[...], preferred_element_type=F32).reshape(8, 16, 128)
        gates[at, :] = jnp.sum(jnp.where(own_lane, pre, 0.0), axis=0)
        score = jnp.dot(key_rows, query_w[...], preferred_element_type=F32).reshape(8, 16, 128)
        scores[at, :] = jnp.sum(jnp.where(own_lane, score, 0.0), axis=0)

    project(here)

    @pl.loop(0, FAR + 10)
    def _(step):
        @pl.when(step < FAR)
        def _():
            far(step).wait_recv()
            along_x(step, 0).start()
            along_x(step, 1).start()

        @pl.when((step >= 4) & (step < FAR + 4))
        def _():
            along_x(step - 4, 0).wait_recv()
            along_x(step - 4, 2).start()

        @pl.when((step >= 8) & (step < FAR + 8))
        def _():
            along_x(step - 8, 1).wait_recv()
            along_x(step - 8, 2).wait_recv()
            swap(step - 8, source(step - 8)).start()

        @pl.when((step >= 6) & (step < 9))
        def _():
            near(step - 6).wait_recv()
            swap(FAR + step - 6, near_source(step - 6)).start()

        @pl.when(step >= 10)
        def _():
            swap(step - 10, source(step - 10)).wait_recv()
            project(source(step - 10))

        @pl.when((step >= 9) & (step < 12))
        def _():
            swap(FAR + step - 9, near_source(step - 9)).wait_recv()
            project(near_source(step - 9))

    lane1 = lax.broadcasted_iota(jnp.int32, (1, 128), 1)
    bias = jnp.where(
        lane1 < 16,
        jnp.where(lane1 < 8, biases[0:1, 0:1], biases[0:1, 1:2]),
        jnp.where(lane1 < 24, biases[1:2, 0:1], biases[1:2, 1:2]),
    )
    pre = gates[...] + bias
    forget = pltpu.roll(jax.nn.log_sigmoid(pre), 112, 1)
    row = lax.broadcasted_iota(jnp.int32, (256, 256), 0)
    col = lax.broadcasted_iota(jnp.int32, (256, 256), 1)
    lower = jnp.where(col < row, 1.0, 0.0)
    before = jnp.dot(lower, forget, preferred_element_type=F32, precision=lax.Precision.HIGHEST)
    total = before[255:256, :] + forget[255:256, :]
    log_weight = pre + jnp.where(lane1 < 8, total - before - forget, before)
    stable = jnp.maximum(total, jnp.max(log_weight, axis=0, keepdims=True))
    weight = jnp.exp(log_weight - stable) * 128.0**-0.5
    stable_out[0:1, :] = stable[:, 0:8]
    stable_out[1:2, :] = pltpu.roll(stable, 120, 1)[:, 0:8]

    read_weight = weight * scores[...]
    denominator = jnp.sum(read_weight, axis=0, keepdims=True)
    floor_value = jnp.maximum(jnp.maximum(jnp.abs(denominator), jnp.exp(-stable)), 1.0)
    read_weight = read_weight / floor_value
    read_weight = read_weight + pltpu.roll(read_weight, 120, 1)
    by_seq = read_weight.T[0:8]
    high = by_seq.astype(BF16)
    both_parts = jnp.concatenate([high.astype(F32), by_seq - high.astype(F32)], axis=0).astype(BF16)
    hidden = []
    for b in range(8):
        two = jnp.dot(both_parts, values[b], preferred_element_type=F32)
        hidden.append(two[b : b + 1] + two[8 + b : 9 + b])
    hidden = jnp.concatenate(hidden, axis=0).astype(BF16)
    head_terms = jnp.dot(hidden, out_w[...], preferred_element_type=F32)
    for t in range(8):
        terms[t] = head_terms[:, 128 * t : 128 * t + 128]

    me = 2 * x + c

    def term(k):
        tx, tc = lax.rem(x + k // 2, 4), lax.rem(c + lax.rem(k, 2), 2)
        return pltpu.make_async_remote_copy(
            src_ref=terms.at[2 * tx + tc],
            dst_ref=parts.at[k],
            send_sem=term_send.at[k],
            recv_sem=term_recv.at[k],
            device_id={"x": tx, "c": tc},
            device_id_type=MESH,
        )

    @pl.loop(1, 8)
    def _(k):
        term(k).start()

    for b in range(8):
        float_keys = keys[b].astype(F32)
        float_values = values[b].astype(F32)
        weighted = []
        for g in range(2):
            spread_weight = jnp.broadcast_to(weight[:, 8 * g + b : 8 * g + b + 1], (256, 128))
            weighted.append((float_values * spread_weight).astype(BF16))
            normal_out[g, b : b + 1, :] = jnp.sum(float_keys * spread_weight, axis=0, keepdims=True)
        cells = lax.dot_general(
            keys[b], jnp.concatenate(weighted, axis=1), (((0,), (0,)), ((), ())), preferred_element_type=F32
        ).astype(BF16)
        memory_out[0, b] = cells[:, :128]
        memory_out[1, b] = cells[:, 128:]

    @pl.loop(0, FAR)
    def _(k):
        far(k).wait_send()
        swap(k, source(k)).wait_send()
        for which in range(3):
            along_x(k, which).wait_send()

    @pl.loop(0, 3)
    def _(k):
        near(k).wait_send()
        swap(FAR + k, near_source(k)).wait_send()

    @pl.loop(1, 8)
    def _(k):
        term(k).wait_recv()

    total_read = terms[me]
    for k in range(1, 8):
        total_read = total_read + parts[k]
    read_out[...] = total_read.astype(BF16)

    @pl.loop(1, 8)
    def _(k):
        term(k).wait_send()


def write_out(memory, normal, stable, read, memory_out, normal_out, stable_out, read_out, sems):
    pairs = ((memory, memory_out), (normal, normal_out), (stable, stable_out), (read, read_out))
    copies = [pltpu.make_async_copy(a, b, sems.at[k]) for k, (a, b) in enumerate(pairs)]
    for copy in copies:
        copy.start()
    for copy in copies:
        copy.wait()


def shards(prompt, w_key, w_value, w_in_gate, w_forget_gate, in_bias, forget_bias, query, w_out):
    vmem = pl.BlockSpec(memory_space=pltpu.VMEM)
    hbm = pl.BlockSpec(memory_space=pltpu.HBM)
    dma = pltpu.SemaphoreType.DMA
    memory, normal, stable, read = pl.pallas_call(
        kernel,
        out_shape=(
            jax.ShapeDtypeStruct((2, 8, 128, 128), BF16),
            jax.ShapeDtypeStruct((2, 8, 128), F32),
            jax.ShapeDtypeStruct((2, 8), F32),
            jax.ShapeDtypeStruct((8, 128), BF16),
        ),
        in_specs=[hbm] * 9,
        out_specs=(vmem, vmem, vmem, vmem),
        scratch_shapes=[
            pltpu.VMEM((16, 8, 16, 1024), BF16),
            pltpu.VMEM((1024, 256), BF16),
            pltpu.VMEM((2, 2, 1024), BF16),
            pltpu.VMEM((1024, 128), BF16),
            pltpu.VMEM((2, 2), F32),
            pltpu.VMEM((8, 128), BF16),
            pltpu.VMEM((128, 128), BF16),
            pltpu.VMEM((128, 1024), BF16),
            pltpu.VMEM((8, 256, 128), BF16),
            pltpu.VMEM((8, 256, 128), BF16),
            pltpu.VMEM((256, 128), F32),
            pltpu.VMEM((256, 128), F32),
            pltpu.VMEM((8, 8, 128), F32),
            pltpu.VMEM((8, 8, 128), F32),
            dma((9,)),
            dma((FAR,)),
            dma((FAR,)),
            dma((3,)),
            dma((3,)),
            dma((FAR, 3)),
            dma((FAR, 3)),
            dma((FAR + 3,)),
            dma((FAR + 3,)),
            dma((8,)),
            dma((8,)),
        ],
        compiler_params=pltpu.CompilerParams(
            collective_id=0, has_side_effects=True, vmem_limit_bytes=20 * 1024 * 1024
        ),
    )(
        *(pltpu.with_memory_space_constraint(v, pltpu.HBM) for v in (
            prompt, w_key[:, 0], w_value[:, 0], w_in_gate[:, :, 0], w_forget_gate[:, :, 0],
            in_bias.T, forget_bias.T, query[:, 0], w_out[0],
        ))
    )
    memory, normal, stable, read = pl.pallas_call(
        write_out,
        out_shape=tuple(jax.ShapeDtypeStruct(v.shape, v.dtype) for v in (memory, normal, stable, read)),
        in_specs=[vmem] * 4,
        out_specs=(hbm,) * 4,
        scratch_shapes=[dma((4,))],
        compiler_params=pltpu.CompilerParams(vmem_limit_bytes=4 * 1024 * 1024),
    )(memory, normal, stable, read)
    return memory[:, :, None], normal[:, :, None], stable[:, :, None], read


def solution(mesh):
    torus = Mesh(
        mesh.devices.reshape(mesh.shape["gr"], 4, 4, 4, 2), ("gr", "z", "y", "x", "c")
    )
    sp = ("z", "y")
    both = ("gr", "z", "y")
    return jax.shard_map(
        shards,
        mesh=torus,
        in_specs=(
            P("gr", sp, None),
            P(None, TP, None),
            P(None, TP, None),
            P(None, None, TP),
            P(None, None, TP),
            P(None, TP),
            P(None, TP),
            P(both, TP, None),
            P(TP, None, None),
        ),
        out_specs=(
            P(None, both, TP, None, None),
            P(None, both, TP, None),
            P(None, both, TP),
            P(both, TP),
        ),
        check_vma=False,
    )
```

```python
import functools

import jax
import jax.numpy as jnp
from jax import lax
from jax.experimental import pallas as pl
from jax.experimental.pallas import tpu as pltpu
from jax.sharding import Mesh
from jax.sharding import PartitionSpec as P

MESH = pl.DeviceIdType.MESH
TP = ("x", "c")
F32 = jnp.float32
BF16 = jnp.bfloat16
FAR = 12


OFFSETS = [(1, 0), (2, 0), (3, 0), (1, 1), (2, 1), (3, 1), (1, 3), (2, 3), (3, 3), (1, 2), (2, 2), (3, 2)]
DIRECT = FAR - 12
NEAR = (1, 3, 2)


def kernel(
    prompt, w_key, w_value, w_in, w_forget, in_bias, forget_bias, query, w_out,
    memory_out, normal_out, stable_out, read_out,
    rows, weights, gate_rows, gate_w, biases, queries, query_w, out_w, keys, values, gates, scores, terms, parts,
    load_sem, far_send, far_recv, line_in, near_send, near_recv, x_send, x_recv, swap_send, swap_recv, term_send, term_recv,
):
    z, y, x, c = (lax.axis_index(a) for a in ("z", "y", "x", "c"))
    here = z * 4 + y
    zs = [z] + [lax.rem(z + k, 4) for k in range(1, 4)]
    ys = [y] + [lax.rem(y + k, 4) for k in range(1, 4)]
    xs = [x] + [lax.rem(x + k, 4) for k in range(1, 4)]
    cs = [c, 1 - c]
    seq = 4 * c + x
    up = lax.rem(x + 1 + 2 * c, 4)
    down = lax.rem(x + 3 + 2 * c, 4)

    loads = [
        pltpu.make_async_copy(w_key, weights.at[:, pl.ds(0, 128)], load_sem.at[0]),
        pltpu.make_async_copy(w_value, weights.at[:, pl.ds(128, 128)], load_sem.at[1]),
        pltpu.make_async_copy(prompt.at[pl.ds(here * 8, 8)], rows.at[here], load_sem.at[2]),
        pltpu.make_async_copy(w_in, gate_rows.at[0], load_sem.at[3]),
        pltpu.make_async_copy(w_forget, gate_rows.at[1], load_sem.at[4]),
        pltpu.make_async_copy(in_bias, biases.at[pl.ds(0, 1)], load_sem.at[5]),
        pltpu.make_async_copy(forget_bias, biases.at[pl.ds(1, 1)], load_sem.at[6]),
        pltpu.make_async_copy(query, queries, load_sem.at[7]),
        pltpu.make_async_copy(w_out, out_w, load_sem.at[8]),
    ]
    for load in loads:
        load.start()

    barrier = pltpu.get_barrier_semaphore()

    for k in range(3, 0, -1):
        pl.semaphore_signal(barrier, inc=1, device_id={"z": zs[k]}, device_id_type=MESH)
        pl.semaphore_signal(barrier, inc=1, device_id={"y": ys[k]}, device_id_type=MESH)
    for k in range(7, 0, -1):
        to = {"x": xs[k // 2], "c": cs[k % 2]}
        pl.semaphore_signal(barrier, inc=1, device_id=to, device_id_type=MESH)

    pl.semaphore_wait(barrier, 13)

    def far(k):
        dz, dy = OFFSETS[k]
        tz, ty = zs[dz], ys[dy]
        return pltpu.make_async_remote_copy(
            src_ref=prompt.at[(tz * 4 + ty) * 8 + seq],
            dst_ref=rows.at[here, seq],
            send_sem=far_send.at[k],
            recv_sem=far_recv.at[k],
            device_id={"z": tz, "y": ty},
            device_id_type=MESH,
        )

    def near(k):
        ty = ys[NEAR[k]]
        return pltpu.make_async_remote_copy(
            src_ref=prompt.at[pl.ds((z * 4 + ty) * 8 + 4 * c, 4)],
            dst_ref=rows.at[here, pl.ds(4 * c, 4)],
            send_sem=near_send.at[k],
            recv_sem=near_recv.at[k],
            device_id={"y": ty},
            device_id_type=MESH,
        )

    def source(k):
        dz, dy = OFFSETS[k]
        return zs[-dz] * 4 + ys[-dy]

    def near_source(k):
        return z * 4 + ys[4 - NEAR[k]]

    def along_x(k, which):
        direct = k >= DIRECT
        block = rows.at[source(k), seq if which < 2 or direct else 4 * c + down]
        return pltpu.make_async_remote_copy(
            src_ref=block,
            dst_ref=block,
            send_sem=x_send.at[k, which],
            recv_sem=x_recv.at[k, which],
            device_id={"x": (up, down, xs[2] if direct else up)[which]},
            device_id_type=MESH,
        )

    def swap(k, src):
        block = rows.at[src, pl.ds(4 * c, 4)]
        return pltpu.make_async_remote_copy(
            src_ref=block,
            dst_ref=block,
            send_sem=swap_send.at[k],
            recv_sem=swap_recv.at[k],
            device_id={"c": cs[1]},
            device_id_type=MESH,
        )

    for k in range(3, 0, -1):
        pl.semaphore_signal(line_in, inc=1, device_id={"y": ys[k]}, device_id_type=MESH)
    for k in range(3):
        far(k).start()

    for load in loads:
        load.wait()

    lane_gate = lax.broadcasted_iota(jnp.int32, (2, 128), 1) // 8
    gate2 = lax.broadcasted_iota(jnp.int32, (2, 128), 0)
    spread_gates = 0.0
    for kind in range(2):
        spread = jnp.where(lane_gate == 2 * kind + gate2, 1.0, 0.0).astype(BF16)
        spread_gates = spread_gates + lax.dot_general(
            gate_rows[kind], spread, (((0,), (0,)), ((), ())), preferred_element_type=F32
        )
    gate_w[...] = spread_gates.astype(BF16)

    lane8 = lax.broadcasted_iota(jnp.int32, (8, 128), 1)
    pick = jnp.where(lax.rem(lane8, 8) == lax.broadcasted_iota(jnp.int32, (8, 128), 0), 1.0, 0.0)
    query_w[...] = lax.dot_general(
        queries[...], pick.astype(BF16), (((0,), (0,)), ((), ())), preferred_element_type=F32
    ).astype(BF16)

    lane = lax.broadcasted_iota(jnp.int32, (8, 16, 128), 2)
    which_seq = lax.broadcasted_iota(jnp.int32, (8, 16, 128), 0)
    own_lane = lax.rem(lane, 8) == which_seq

    def project(src):
        block = rows[src].reshape(128, 1024)
        both = jnp.dot(block, weights[...], preferred_element_type=F32)
        at = pl.ds(pl.multiple_of(src * 16, 16), 16)
        key_rows = both[:, :128].astype(BF16)
        keys[:, at, :] = key_rows.reshape(8, 16, 128)
        values[:, at, :] = both[:, 128:].astype(BF16).reshape(8, 16, 128)
        pre = jnp.dot(block, gate_w[...], preferred_element_type=F32).reshape(8, 16, 128)
        gates[at, :] = jnp.sum(jnp.where(own_lane, pre, 0.0), axis=0)
        score = jnp.dot(key_rows, query_w[...], preferred_element_type=F32).reshape(8, 16, 128)
        scores[at, :] = jnp.sum(jnp.where(own_lane, score, 0.0), axis=0)

    project(here)
    pl.semaphore_wait(line_in, 3)
    for k in range(3, 4):
        far(k).start()

    def arrive(k):
        far(k).wait_recv()
        along_x(k, 0).start()
        along_x(k, 1).start()
        if k >= DIRECT:
            along_x(k, 2).start()
        if k + 4 < FAR:
            far(k + 4).start()

    def relay(k):
        along_x(k, 0).wait_recv()
        along_x(k, 2).start()

    def start_swap(k):
        if k >= DIRECT:
            along_x(k, 0).wait_recv()
        along_x(k, 1).wait_recv()
        along_x(k, 2).wait_recv()
        swap(k, source(k)).start()

    def finish(k):
        swap(k, source(k)).wait_recv()
        project(source(k))

    def start_near(k):
        near(k).start()

    def swap_near(k):
        near(k).wait_recv()
        swap(FAR + k, near_source(k)).start()

    def finish_near(k):
        swap(FAR + k, near_source(k)).wait_recv()
        project(near_source(k))

    events = []
    for k in range(FAR):
        events.append((k, 0, arrive, k))
        if k < DIRECT:
            events.append((k + 3, 2, relay, k))
        events.append((k + 8, 3, start_swap, k))
        events.append((k + 10, 4, finish, k))
    for k in range(3):
        if (2, 2, 4)[k]:
            events.append(((2, 2, 4)[k], 5, start_near, k))
        events.append(((6, 8, 10)[k], 6, swap_near, k))
        events.append(((9, 11, 13)[k], 7, finish_near, k))
    for _, _, stage, k in sorted(events, key=lambda e: (e[0], e[1], e[3])):
        stage(k)

    lane1 = lax.broadcasted_iota(jnp.int32, (1, 128), 1)
    bias = jnp.where(
        lane1 < 16,
        jnp.where(lane1 < 8, biases[0:1, 0:1], biases[0:1, 1:2]),
        jnp.where(lane1 < 24, biases[1:2, 0:1], biases[1:2, 1:2]),
    )
    pre = gates[...] + bias
    forget = pltpu.roll(jax.nn.log_sigmoid(pre), 112, 1)
    row = lax.broadcasted_iota(jnp.int32, (256, 256), 0)
    col = lax.broadcasted_iota(jnp.int32, (256, 256), 1)
    lower = jnp.where(col < row, 1.0, 0.0)
    before = jnp.dot(lower, forget, preferred_element_type=F32, precision=lax.Precision.HIGHEST)
    total = before[255:256, :] + forget[255:256, :]
    log_weight = pre + jnp.where(lane1 < 8, total - before - forget, before)
    stable = jnp.maximum(total, jnp.max(log_weight, axis=0, keepdims=True))
    weight = jnp.exp(log_weight - stable) * 128.0**-0.5
    stable_out[0:1, :] = stable[:, 0:8]
    stable_out[1:2, :] = pltpu.roll(stable, 120, 1)[:, 0:8]

    read_weight = weight * scores[...]
    denominator = jnp.sum(read_weight, axis=0, keepdims=True)
    floor_value = jnp.maximum(jnp.maximum(jnp.abs(denominator), jnp.exp(-stable)), 1.0)
    read_weight = read_weight / floor_value
    read_weight = read_weight + pltpu.roll(read_weight, 120, 1)
    by_seq = read_weight.T[0:8]
    high = by_seq.astype(BF16)
    both_parts = jnp.concatenate([high.astype(F32), by_seq - high.astype(F32)], axis=0).astype(BF16)
    hidden = []
    for b in range(8):
        two = jnp.dot(both_parts, values[b], preferred_element_type=F32)
        hidden.append(two[b : b + 1] + two[8 + b : 9 + b])
    hidden = jnp.concatenate(hidden, axis=0).astype(BF16)
    head_terms = jnp.dot(hidden, out_w[...], preferred_element_type=F32)
    for t in range(8):
        terms[t] = head_terms[:, 128 * t : 128 * t + 128]

    me = 2 * x + c

    def term(k):
        tx, tc = xs[k // 2], cs[k % 2]
        return pltpu.make_async_remote_copy(
            src_ref=terms.at[2 * tx + tc],
            dst_ref=parts.at[k],
            send_sem=term_send.at[k],
            recv_sem=term_recv.at[k],
            device_id={"x": tx, "c": tc},
            device_id_type=MESH,
        )

    for k in range(1, 8):
        term(k).start()

    for b in range(8):
        float_keys = keys[b].astype(F32)
        float_values = values[b].astype(F32)
        weighted = []
        for g in range(2):
            spread_weight = jnp.broadcast_to(weight[:, 8 * g + b : 8 * g + b + 1], (256, 128))
            weighted.append((float_values * spread_weight).astype(BF16))
            normal_out[g, b : b + 1, :] = jnp.sum(float_keys * spread_weight, axis=0, keepdims=True)
        cells = lax.dot_general(
            keys[b], jnp.concatenate(weighted, axis=1), (((0,), (0,)), ((), ())), preferred_element_type=F32
        ).astype(BF16)
        memory_out[0, b] = cells[:, :128]
        memory_out[1, b] = cells[:, 128:]

    for k in range(FAR):
        far(k).wait_send()
        swap(k, source(k)).wait_send()
        for which in range(3):
            along_x(k, which).wait_send()

    for k in range(3):
        near(k).wait_send()
        swap(FAR + k, near_source(k)).wait_send()

    for k in range(1, 8):
        term(k).wait_recv()

    total_read = terms[me]
    for k in range(1, 8):
        total_read = total_read + parts[k]
    read_out[...] = total_read.astype(BF16)

    for k in range(1, 8):
        term(k).wait_send()


def write_out(memory, normal, stable, read, memory_out, normal_out, stable_out, read_out, sems):
    pairs = ((memory, memory_out), (normal, normal_out), (stable, stable_out), (read, read_out))
    copies = [pltpu.make_async_copy(a, b, sems.at[k]) for k, (a, b) in enumerate(pairs)]
    for copy in copies:
        copy.start()
    for copy in copies:
        copy.wait()


def shards(prompt, w_key, w_value, w_in_gate, w_forget_gate, in_bias, forget_bias, query, w_out):
    vmem = pl.BlockSpec(memory_space=pltpu.VMEM)
    hbm = pl.BlockSpec(memory_space=pltpu.HBM)
    dma = pltpu.SemaphoreType.DMA
    memory, normal, stable, read = pl.pallas_call(
        kernel,
        out_shape=(
            jax.ShapeDtypeStruct((2, 8, 128, 128), BF16),
            jax.ShapeDtypeStruct((2, 8, 128), F32),
            jax.ShapeDtypeStruct((2, 8), F32),
            jax.ShapeDtypeStruct((8, 128), BF16),
        ),
        in_specs=[hbm] * 9,
        out_specs=(vmem, vmem, vmem, vmem),
        scratch_shapes=[
            pltpu.VMEM((16, 8, 16, 1024), BF16),
            pltpu.VMEM((1024, 256), BF16),
            pltpu.VMEM((2, 2, 1024), BF16),
            pltpu.VMEM((1024, 128), BF16),
            pltpu.VMEM((2, 2), F32),
            pltpu.VMEM((8, 128), BF16),
            pltpu.VMEM((128, 128), BF16),
            pltpu.VMEM((128, 1024), BF16),
            pltpu.VMEM((8, 256, 128), BF16),
            pltpu.VMEM((8, 256, 128), BF16),
            pltpu.VMEM((256, 128), F32),
            pltpu.VMEM((256, 128), F32),
            pltpu.VMEM((8, 8, 128), F32),
            pltpu.VMEM((8, 8, 128), F32),
            dma((9,)),
            dma((FAR,)),
            dma((FAR,)),
            pltpu.SemaphoreType.REGULAR,
            dma((3,)),
            dma((3,)),
            dma((FAR, 3)),
            dma((FAR, 3)),
            dma((FAR + 3,)),
            dma((FAR + 3,)),
            dma((8,)),
            dma((8,)),
        ],
        compiler_params=pltpu.CompilerParams(
            collective_id=0, has_side_effects=True, vmem_limit_bytes=20 * 1024 * 1024
        ),
    )(
        *(pltpu.with_memory_space_constraint(v, pltpu.HBM) for v in (
            prompt, w_key[:, 0], w_value[:, 0], w_in_gate[:, :, 0], w_forget_gate[:, :, 0],
            in_bias.T, forget_bias.T, query[:, 0], w_out[0],
        ))
    )
    memory, normal, stable, read = pl.pallas_call(
        write_out,
        out_shape=tuple(jax.ShapeDtypeStruct(v.shape, v.dtype) for v in (memory, normal, stable, read)),
        in_specs=[vmem] * 4,
        out_specs=(hbm,) * 4,
        scratch_shapes=[dma((4,))],
        compiler_params=pltpu.CompilerParams(vmem_limit_bytes=4 * 1024 * 1024),
    )(memory, normal, stable, read)
    return memory[:, :, None], normal[:, :, None], stable[:, :, None], read


def solution(mesh):
    torus = Mesh(
        mesh.devices.reshape(mesh.shape["gr"], 4, 4, 4, 2), ("gr", "z", "y", "x", "c")
    )
    sp = ("z", "y")
    both = ("gr", "z", "y")
    return jax.shard_map(
        shards,
        mesh=torus,
        in_specs=(
            P("gr", sp, None),
            P(None, TP, None),
            P(None, TP, None),
            P(None, None, TP),
            P(None, None, TP),
            P(None, TP),
            P(None, TP),
            P(both, TP, None),
            P(TP, None, None),
        ),
        out_specs=(
            P(None, both, TP, None, None),
            P(None, both, TP, None),
            P(None, both, TP),
            P(both, TP),
        ),
        check_vma=False,
    )
```

```python
import functools

import jax
import jax.numpy as jnp
from jax import lax
from jax.experimental import pallas as pl
from jax.experimental.pallas import tpu as pltpu
from jax.sharding import Mesh
from jax.sharding import PartitionSpec as P

MESH = pl.DeviceIdType.MESH
TP = ("x", "c")
F32 = jnp.float32
BF16 = jnp.bfloat16
FAR = 8


OFFSETS = [(2, 0), (2, 1), (3, 1), (1, 3), (2, 3), (1, 2), (2, 2), (3, 2)]
MADE = [(1, 0), (3, 0), (1, 1), (3, 3)]
DIRECT = FAR - 8
NEAR = (1, 3, 2)


def kernel(
    prompt, w_key, w_value, w_in, w_forget, in_bias, forget_bias, query, w_out,
    memory_out, normal_out, stable_out, read_out,
    rows, weights, gate_rows, gate_w, biases, queries, query_w, out_w, keys, values, gates, scores, made_rows, made_keys, made_values, made_gates, terms, parts,
    load_sem, far_send, far_recv, line_in, made_send, made_recv, near_send, near_recv, x_send, x_recv, swap_send, swap_recv, term_send, term_recv,
):
    z, y, x, c = (lax.axis_index(a) for a in ("z", "y", "x", "c"))
    here = z * 4 + y
    zs = [z] + [lax.rem(z + k, 4) for k in range(1, 4)]
    ys = [y] + [lax.rem(y + k, 4) for k in range(1, 4)]
    xs = [x] + [lax.rem(x + k, 4) for k in range(1, 4)]
    cs = [c, 1 - c]
    seq = 4 * c + x
    up = lax.rem(x + 1 + 2 * c, 4)
    down = lax.rem(x + 3 + 2 * c, 4)

    loads = [
        pltpu.make_async_copy(w_key, weights.at[:, pl.ds(0, 128)], load_sem.at[0]),
        pltpu.make_async_copy(w_value, weights.at[:, pl.ds(128, 128)], load_sem.at[1]),
        pltpu.make_async_copy(prompt.at[pl.ds(here * 8, 8)], rows.at[here], load_sem.at[2]),
        pltpu.make_async_copy(w_in, gate_rows.at[0], load_sem.at[3]),
        pltpu.make_async_copy(w_forget, gate_rows.at[1], load_sem.at[4]),
        pltpu.make_async_copy(in_bias, biases.at[pl.ds(0, 1)], load_sem.at[5]),
        pltpu.make_async_copy(forget_bias, biases.at[pl.ds(1, 1)], load_sem.at[6]),
        pltpu.make_async_copy(query, queries, load_sem.at[7]),
        pltpu.make_async_copy(w_out, out_w, load_sem.at[8]),
    ]
    for q, (dz, dy) in enumerate(MADE):
        there = (zs[dz] * 4 + ys[dy]) * 8
        loads.append(pltpu.make_async_copy(prompt.at[pl.ds(there, 8)], made_rows.at[q], load_sem.at[9 + q]))
    for load in loads:
        load.start()

    barrier = pltpu.get_barrier_semaphore()

    for k in range(3, 0, -1):
        pl.semaphore_signal(barrier, inc=1, device_id={"z": zs[k]}, device_id_type=MESH)
        pl.semaphore_signal(barrier, inc=1, device_id={"y": ys[k]}, device_id_type=MESH)
    for k in range(7, 0, -1):
        to = {"x": xs[k // 2], "c": cs[k % 2]}
        pl.semaphore_signal(barrier, inc=1, device_id=to, device_id_type=MESH)

    pl.semaphore_wait(barrier, 13)

    def far(k):
        dz, dy = OFFSETS[k]
        tz, ty = zs[dz], ys[dy]
        return pltpu.make_async_remote_copy(
            src_ref=prompt.at[(tz * 4 + ty) * 8 + seq],
            dst_ref=rows.at[here, seq],
            send_sem=far_send.at[k],
            recv_sem=far_recv.at[k],
            device_id={"z": tz, "y": ty},
            device_id_type=MESH,
        )

    def near(k):
        ty = ys[NEAR[k]]
        return pltpu.make_async_remote_copy(
            src_ref=prompt.at[pl.ds((z * 4 + ty) * 8 + 4 * c, 4)],
            dst_ref=rows.at[here, pl.ds(4 * c, 4)],
            send_sem=near_send.at[k],
            recv_sem=near_recv.at[k],
            device_id={"y": ty},
            device_id_type=MESH,
        )

    def source(k):
        dz, dy = OFFSETS[k]
        return zs[-dz] * 4 + ys[-dy]

    def near_source(k):
        return z * 4 + ys[4 - NEAR[k]]

    def along_x(k, which):
        direct = k >= DIRECT
        block = rows.at[source(k), seq if which < 2 or direct else 4 * c + down]
        return pltpu.make_async_remote_copy(
            src_ref=block,
            dst_ref=block,
            send_sem=x_send.at[k, which],
            recv_sem=x_recv.at[k, which],
            device_id={"x": (up, down, xs[2] if direct else up)[which]},
            device_id_type=MESH,
        )

    def swap(k, src):
        block = rows.at[src, pl.ds(4 * c, 4)]
        return pltpu.make_async_remote_copy(
            src_ref=block,
            dst_ref=block,
            send_sem=swap_send.at[k],
            recv_sem=swap_recv.at[k],
            device_id={"c": cs[1]},
            device_id_type=MESH,
        )

    for k in range(3, 0, -1):
        pl.semaphore_signal(line_in, inc=1, device_id={"y": ys[k]}, device_id_type=MESH)
    for k in range(1):
        far(k).start()

    for load in loads:
        load.wait()

    lane_gate = lax.broadcasted_iota(jnp.int32, (2, 128), 1) // 8
    gate2 = lax.broadcasted_iota(jnp.int32, (2, 128), 0)
    spread_gates = 0.0
    for kind in range(2):
        spread = jnp.where(lane_gate == 2 * kind + gate2, 1.0, 0.0).astype(BF16)
        spread_gates = spread_gates + lax.dot_general(
            gate_rows[kind], spread, (((0,), (0,)), ((), ())), preferred_element_type=F32
        )
    gate_w[...] = spread_gates.astype(BF16)

    lane8 = lax.broadcasted_iota(jnp.int32, (8, 128), 1)
    pick = jnp.where(lax.rem(lane8, 8) == lax.broadcasted_iota(jnp.int32, (8, 128), 0), 1.0, 0.0)
    query_w[...] = lax.dot_general(
        queries[...], pick.astype(BF16), (((0,), (0,)), ((), ())), preferred_element_type=F32
    ).astype(BF16)

    lane = lax.broadcasted_iota(jnp.int32, (8, 16, 128), 2)
    which_seq = lax.broadcasted_iota(jnp.int32, (8, 16, 128), 0)
    own_lane = lax.rem(lane, 8) == which_seq

    def products(block):
        both = jnp.dot(block, weights[...], preferred_element_type=F32)
        pre = jnp.dot(block, gate_w[...], preferred_element_type=F32).reshape(8, 16, 128)
        return both, jnp.sum(jnp.where(own_lane, pre, 0.0), axis=0)

    def positions(src):
        return pl.ds(pl.multiple_of(src * 16, 16), 16)

    def score(src, key_rows):
        every = jnp.dot(key_rows, query_w[...], preferred_element_type=F32).reshape(8, 16, 128)
        scores[positions(src), :] = jnp.sum(jnp.where(own_lane, every, 0.0), axis=0)

    def project(src):
        both, pre = products(rows[src].reshape(128, 1024))
        at = positions(src)
        key_rows = both[:, :128].astype(BF16)
        keys[:, at, :] = key_rows.reshape(8, 16, 128)
        values[:, at, :] = both[:, 128:].astype(BF16).reshape(8, 16, 128)
        gates[at, :] = pre
        score(src, key_rows)

    def made(q, which):
        dz, dy = MADE[q]
        at = positions(here)
        src, dst = (
            (made_keys.at[q], keys.at[:, at, :]),
            (made_values.at[q], values.at[:, at, :]),
            (made_gates.at[q], gates.at[at, :]),
        )[which]
        return pltpu.make_async_remote_copy(
            src_ref=src,
            dst_ref=dst,
            send_sem=made_send.at[q, which],
            recv_sem=made_recv.at[q, which],
            device_id={"z": zs[dz], "y": ys[dy]},
            device_id_type=MESH,
        )

    def make(q):
        both, pre = products(made_rows[q].reshape(128, 1024))
        made_keys[q] = both[:, :128].astype(BF16).reshape(8, 16, 128)
        made_values[q] = both[:, 128:].astype(BF16).reshape(8, 16, 128)
        made_gates[q] = pre

    def send_made(q):
        for which in range(3):
            made(q, which).start()

    def finish_made(q):
        for which in range(3):
            made(q, which).wait_recv()
        src = zs[-MADE[q][0]] * 4 + ys[-MADE[q][1]]
        score(src, keys[:, positions(src), :].reshape(128, 128))

    project(here)
    pl.semaphore_wait(line_in, 3)
    for k in range(1, 5):
        far(k).start()

    def arrive(k):
        far(k).wait_recv()
        along_x(k, 0).start()
        along_x(k, 1).start()
        if k >= DIRECT:
            along_x(k, 2).start()
        if k + 5 < FAR:
            far(k + 5).start()

    def relay(k):
        along_x(k, 0).wait_recv()
        along_x(k, 2).start()

    def start_swap(k):
        if k >= DIRECT:
            along_x(k, 0).wait_recv()
        along_x(k, 1).wait_recv()
        along_x(k, 2).wait_recv()
        swap(k, source(k)).start()

    def finish(k):
        swap(k, source(k)).wait_recv()
        project(source(k))

    def start_near(k):
        near(k).start()

    def swap_near(k):
        near(k).wait_recv()
        swap(FAR + k, near_source(k)).start()

    def finish_near(k):
        swap(FAR + k, near_source(k)).wait_recv()
        project(near_source(k))

    events = []
    for k in range(FAR):
        events.append((k, 0, arrive, k))
        if k < DIRECT:
            events.append((k + 3, 2, relay, k))
        events.append((k + 8, 3, start_swap, k))
        events.append((k + 10, 4, finish, k))
    for k in range(3):
        if (1, 1, 3)[k]:
            events.append(((1, 1, 3)[k], 5, start_near, k))
        events.append(((6, 7, 8)[k], 6, swap_near, k))
        events.append(((9, 10, 11)[k], 7, finish_near, k))
    for q in range(len(MADE)):
        events.append(((-1, 0, 1, 2)[q], 7, make, q))
        events.append(((5, 5, 6, 7)[q], 8, send_made, q))
        events.append(((12, 13, 14, 15)[q], 9, finish_made, q))
    for _, _, stage, k in sorted(events, key=lambda e: (e[0], e[1], e[3])):
        stage(k)

    lane1 = lax.broadcasted_iota(jnp.int32, (1, 128), 1)
    bias = jnp.where(
        lane1 < 16,
        jnp.where(lane1 < 8, biases[0:1, 0:1], biases[0:1, 1:2]),
        jnp.where(lane1 < 24, biases[1:2, 0:1], biases[1:2, 1:2]),
    )
    pre = gates[...] + bias
    forget = pltpu.roll(jax.nn.log_sigmoid(pre), 112, 1)
    row = lax.broadcasted_iota(jnp.int32, (256, 256), 0)
    col = lax.broadcasted_iota(jnp.int32, (256, 256), 1)
    lower = jnp.where(col < row, 1.0, 0.0)
    before = jnp.dot(lower, forget, preferred_element_type=F32, precision=lax.Precision.HIGHEST)
    total = before[255:256, :] + forget[255:256, :]
    log_weight = pre + jnp.where(lane1 < 8, total - before - forget, before)
    stable = jnp.maximum(total, jnp.max(log_weight, axis=0, keepdims=True))
    weight = jnp.exp(log_weight - stable) * 128.0**-0.5
    stable_out[0:1, :] = stable[:, 0:8]
    stable_out[1:2, :] = pltpu.roll(stable, 120, 1)[:, 0:8]

    read_weight = weight * scores[...]
    denominator = jnp.sum(read_weight, axis=0, keepdims=True)
    floor_value = jnp.maximum(jnp.maximum(jnp.abs(denominator), jnp.exp(-stable)), 1.0)
    read_weight = read_weight / floor_value
    read_weight = read_weight + pltpu.roll(read_weight, 120, 1)
    by_seq = read_weight.T[0:8]
    high = by_seq.astype(BF16)
    both_parts = jnp.concatenate([high.astype(F32), by_seq - high.astype(F32)], axis=0).astype(BF16)
    hidden = []
    for b in range(8):
        two = jnp.dot(both_parts, values[b], preferred_element_type=F32)
        hidden.append(two[b : b + 1] + two[8 + b : 9 + b])
    hidden = jnp.concatenate(hidden, axis=0).astype(BF16)
    head_terms = jnp.dot(hidden, out_w[...], preferred_element_type=F32)
    for t in range(8):
        terms[t] = head_terms[:, 128 * t : 128 * t + 128]

    me = 2 * x + c

    def term(k):
        tx, tc = xs[k // 2], cs[k % 2]
        return pltpu.make_async_remote_copy(
            src_ref=terms.at[2 * tx + tc],
            dst_ref=parts.at[k],
            send_sem=term_send.at[k],
            recv_sem=term_recv.at[k],
            device_id={"x": tx, "c": tc},
            device_id_type=MESH,
        )

    for k in range(1, 8):
        term(k).start()

    for b in range(8):
        float_keys = keys[b].astype(F32)
        float_values = values[b].astype(F32)
        weighted = []
        for g in range(2):
            spread_weight = jnp.broadcast_to(weight[:, 8 * g + b : 8 * g + b + 1], (256, 128))
            weighted.append((float_values * spread_weight).astype(BF16))
            normal_out[g, b : b + 1, :] = jnp.sum(float_keys * spread_weight, axis=0, keepdims=True)
        cells = lax.dot_general(
            keys[b], jnp.concatenate(weighted, axis=1), (((0,), (0,)), ((), ())), preferred_element_type=F32
        ).astype(BF16)
        memory_out[0, b] = cells[:, :128]
        memory_out[1, b] = cells[:, 128:]

    for k in range(FAR):
        far(k).wait_send()
        swap(k, source(k)).wait_send()
        for which in range(3):
            along_x(k, which).wait_send()

    for q in range(len(MADE)):
        for which in range(3):
            made(q, which).wait_send()
    for k in range(3):
        near(k).wait_send()
        swap(FAR + k, near_source(k)).wait_send()

    for k in range(1, 8):
        term(k).wait_recv()

    total_read = terms[me]
    for k in range(1, 8):
        total_read = total_read + parts[k]
    read_out[...] = total_read.astype(BF16)

    for k in range(1, 8):
        term(k).wait_send()


def write_out(memory, normal, stable, read, memory_out, normal_out, stable_out, read_out, sems):
    pairs = ((memory, memory_out), (normal, normal_out), (stable, stable_out), (read, read_out))
    copies = [pltpu.make_async_copy(a, b, sems.at[k]) for k, (a, b) in enumerate(pairs)]
    for copy in copies:
        copy.start()
    for copy in copies:
        copy.wait()


def shards(prompt, w_key, w_value, w_in_gate, w_forget_gate, in_bias, forget_bias, query, w_out):
    vmem = pl.BlockSpec(memory_space=pltpu.VMEM)
    hbm = pl.BlockSpec(memory_space=pltpu.HBM)
    dma = pltpu.SemaphoreType.DMA
    memory, normal, stable, read = pl.pallas_call(
        kernel,
        out_shape=(
            jax.ShapeDtypeStruct((2, 8, 128, 128), BF16),
            jax.ShapeDtypeStruct((2, 8, 128), F32),
            jax.ShapeDtypeStruct((2, 8), F32),
            jax.ShapeDtypeStruct((8, 128), BF16),
        ),
        in_specs=[hbm] * 9,
        out_specs=(vmem, vmem, vmem, vmem),
        scratch_shapes=[
            pltpu.VMEM((16, 8, 16, 1024), BF16),
            pltpu.VMEM((1024, 256), BF16),
            pltpu.VMEM((2, 2, 1024), BF16),
            pltpu.VMEM((1024, 128), BF16),
            pltpu.VMEM((2, 2), F32),
            pltpu.VMEM((8, 128), BF16),
            pltpu.VMEM((128, 128), BF16),
            pltpu.VMEM((128, 1024), BF16),
            pltpu.VMEM((8, 256, 128), BF16),
            pltpu.VMEM((8, 256, 128), BF16),
            pltpu.VMEM((256, 128), F32),
            pltpu.VMEM((256, 128), F32),
            pltpu.VMEM((4, 8, 16, 1024), BF16),
            pltpu.VMEM((4, 8, 16, 128), BF16),
            pltpu.VMEM((4, 8, 16, 128), BF16),
            pltpu.VMEM((4, 16, 128), F32),
            pltpu.VMEM((8, 8, 128), F32),
            pltpu.VMEM((8, 8, 128), F32),
            dma((13,)),
            dma((FAR,)),
            dma((FAR,)),
            pltpu.SemaphoreType.REGULAR,
            dma((4, 3)),
            dma((4, 3)),
            dma((3,)),
            dma((3,)),
            dma((FAR, 3)),
            dma((FAR, 3)),
            dma((FAR + 3,)),
            dma((FAR + 3,)),
            dma((8,)),
            dma((8,)),
        ],
        compiler_params=pltpu.CompilerParams(
            collective_id=0, has_side_effects=True, vmem_limit_bytes=20 * 1024 * 1024
        ),
    )(
        *(pltpu.with_memory_space_constraint(v, pltpu.HBM) for v in (
            prompt, w_key[:, 0], w_value[:, 0], w_in_gate[:, :, 0], w_forget_gate[:, :, 0],
            in_bias.T, forget_bias.T, query[:, 0], w_out[0],
        ))
    )
    memory, normal, stable, read = pl.pallas_call(
        write_out,
        out_shape=tuple(jax.ShapeDtypeStruct(v.shape, v.dtype) for v in (memory, normal, stable, read)),
        in_specs=[vmem] * 4,
        out_specs=(hbm,) * 4,
        scratch_shapes=[dma((4,))],
        compiler_params=pltpu.CompilerParams(vmem_limit_bytes=4 * 1024 * 1024),
    )(memory, normal, stable, read)
    return memory[:, :, None], normal[:, :, None], stable[:, :, None], read


def solution(mesh):
    torus = Mesh(
        mesh.devices.reshape(mesh.shape["gr"], 4, 4, 4, 2), ("gr", "z", "y", "x", "c")
    )
    sp = ("z", "y")
    both = ("gr", "z", "y")
    return jax.shard_map(
        shards,
        mesh=torus,
        in_specs=(
            P("gr", sp, None),
            P(None, TP, None),
            P(None, TP, None),
            P(None, None, TP),
            P(None, None, TP),
            P(None, TP),
            P(None, TP),
            P(both, TP, None),
            P(TP, None, None),
        ),
        out_specs=(
            P(None, both, TP, None, None),
            P(None, both, TP, None),
            P(None, both, TP),
            P(both, TP),
        ),
        check_vma=False,
    )
```

```python
import functools

import jax
import jax.numpy as jnp
from jax import lax
from jax.experimental import pallas as pl
from jax.experimental.pallas import tpu as pltpu
from jax.sharding import Mesh
from jax.sharding import PartitionSpec as P

MESH = pl.DeviceIdType.MESH
TP = ("x", "c")
F32 = jnp.float32
BF16 = jnp.bfloat16
FAR = 8


OFFSETS = [(2, 0), (2, 1), (3, 1), (1, 3), (2, 3), (1, 2), (2, 2), (3, 2)]
MADE = [(1, 0), (3, 0), (1, 1), (3, 3)]
DIRECT = FAR - 8
NEAR = (1, 3, 2)


def kernel(
    prompt, w_key, w_value, w_in, w_forget, in_bias, forget_bias, query, w_out,
    memory_out, normal_out, stable_out, read_out,
    rows, weights, gate_rows, gate_w, biases, queries, query_w, out_w, keys, values, gates, scores, made_rows, made_keys, made_values, made_gates, terms, parts,
    load_sem, far_send, far_recv, line_in, made_send, made_recv, near_send, near_recv, x_send, x_recv, swap_send, swap_recv, term_send, term_recv,
):
    z, y, x, c = (lax.axis_index(a) for a in ("z", "y", "x", "c"))
    here = z * 4 + y
    zs = [z] + [lax.rem(z + k, 4) for k in range(1, 4)]
    ys = [y] + [lax.rem(y + k, 4) for k in range(1, 4)]
    xs = [x] + [lax.rem(x + k, 4) for k in range(1, 4)]
    cs = [c, 1 - c]
    seq = 4 * c + x
    up = lax.rem(x + 1 + 2 * c, 4)
    down = lax.rem(x + 3 + 2 * c, 4)

    loads = [
        pltpu.make_async_copy(w_key, weights.at[:, pl.ds(0, 128)], load_sem.at[0]),
        pltpu.make_async_copy(w_value, weights.at[:, pl.ds(128, 128)], load_sem.at[1]),
        pltpu.make_async_copy(prompt.at[pl.ds(here * 8, 8)], rows.at[here], load_sem.at[2]),
        pltpu.make_async_copy(w_in, gate_rows.at[0], load_sem.at[3]),
        pltpu.make_async_copy(w_forget, gate_rows.at[1], load_sem.at[4]),
        pltpu.make_async_copy(in_bias, biases.at[pl.ds(0, 1)], load_sem.at[5]),
        pltpu.make_async_copy(forget_bias, biases.at[pl.ds(1, 1)], load_sem.at[6]),
        pltpu.make_async_copy(query, queries, load_sem.at[7]),
        pltpu.make_async_copy(w_out, out_w, load_sem.at[8]),
    ]
    for q, (dz, dy) in enumerate(MADE):
        there = (zs[dz] * 4 + ys[dy]) * 8
        loads.append(pltpu.make_async_copy(prompt.at[pl.ds(there, 8)], made_rows.at[q], load_sem.at[9 + q]))
    for load in loads:
        load.start()

    barrier = pltpu.get_barrier_semaphore()

    for k in range(3, 0, -1):
        pl.semaphore_signal(barrier, inc=1, device_id={"z": zs[k]}, device_id_type=MESH)
        pl.semaphore_signal(barrier, inc=1, device_id={"y": ys[k]}, device_id_type=MESH)
    for k in range(7, 0, -1):
        to = {"x": xs[k // 2], "c": cs[k % 2]}
        pl.semaphore_signal(barrier, inc=1, device_id=to, device_id_type=MESH)

    pl.semaphore_wait(barrier, 13)

    def far(k):
        dz, dy = OFFSETS[k]
        tz, ty = zs[dz], ys[dy]
        return pltpu.make_async_remote_copy(
            src_ref=prompt.at[(tz * 4 + ty) * 8 + seq],
            dst_ref=rows.at[here, seq],
            send_sem=far_send.at[k],
            recv_sem=far_recv.at[k],
            device_id={"z": tz, "y": ty},
            device_id_type=MESH,
        )

    def near(k):
        ty = ys[NEAR[k]]
        return pltpu.make_async_remote_copy(
            src_ref=prompt.at[pl.ds((z * 4 + ty) * 8 + 4 * c, 4)],
            dst_ref=rows.at[here, pl.ds(4 * c, 4)],
            send_sem=near_send.at[k],
            recv_sem=near_recv.at[k],
            device_id={"y": ty},
            device_id_type=MESH,
        )

    def source(k):
        dz, dy = OFFSETS[k]
        return zs[-dz] * 4 + ys[-dy]

    def near_source(k):
        return z * 4 + ys[4 - NEAR[k]]

    def along_x(k, which):
        direct = k >= DIRECT
        block = rows.at[source(k), seq if which < 2 or direct else 4 * c + down]
        return pltpu.make_async_remote_copy(
            src_ref=block,
            dst_ref=block,
            send_sem=x_send.at[k, which],
            recv_sem=x_recv.at[k, which],
            device_id={"x": (up, down, xs[2] if direct else up)[which]},
            device_id_type=MESH,
        )

    def swap(k, src):
        block = rows.at[src, pl.ds(4 * c, 4)]
        return pltpu.make_async_remote_copy(
            src_ref=block,
            dst_ref=block,
            send_sem=swap_send.at[k],
            recv_sem=swap_recv.at[k],
            device_id={"c": cs[1]},
            device_id_type=MESH,
        )

    for k in range(3, 0, -1):
        pl.semaphore_signal(line_in, inc=1, device_id={"y": ys[k]}, device_id_type=MESH)
    for k in range(1):
        far(k).start()
    near(0).start()
    near(1).start()
    near(2).start()

    for load in loads:
        load.wait()

    lane_gate = lax.broadcasted_iota(jnp.int32, (2, 128), 1) // 8
    gate2 = lax.broadcasted_iota(jnp.int32, (2, 128), 0)
    spread_gates = 0.0
    for kind in range(2):
        spread = jnp.where(lane_gate == 2 * kind + gate2, 1.0, 0.0).astype(BF16)
        spread_gates = spread_gates + lax.dot_general(
            gate_rows[kind], spread, (((0,), (0,)), ((), ())), preferred_element_type=F32
        )
    gate_w[...] = spread_gates.astype(BF16)

    lane8 = lax.broadcasted_iota(jnp.int32, (8, 128), 1)
    pick = jnp.where(lax.rem(lane8, 8) == lax.broadcasted_iota(jnp.int32, (8, 128), 0), 1.0, 0.0)
    query_w[...] = lax.dot_general(
        queries[...], pick.astype(BF16), (((0,), (0,)), ((), ())), preferred_element_type=F32
    ).astype(BF16)

    lane = lax.broadcasted_iota(jnp.int32, (8, 16, 128), 2)
    which_seq = lax.broadcasted_iota(jnp.int32, (8, 16, 128), 0)
    own_lane = lax.rem(lane, 8) == which_seq

    def products(block):
        both = jnp.dot(block, weights[...], preferred_element_type=F32)
        pre = jnp.dot(block, gate_w[...], preferred_element_type=F32).reshape(8, 16, 128)
        return both, jnp.sum(jnp.where(own_lane, pre, 0.0), axis=0)

    def positions(src):
        return pl.ds(pl.multiple_of(src * 16, 16), 16)

    def score(src, key_rows):
        every = jnp.dot(key_rows, query_w[...], preferred_element_type=F32).reshape(8, 16, 128)
        scores[positions(src), :] = jnp.sum(jnp.where(own_lane, every, 0.0), axis=0)

    def project(src):
        both, pre = products(rows[src].reshape(128, 1024))
        at = positions(src)
        key_rows = both[:, :128].astype(BF16)
        keys[:, at, :] = key_rows.reshape(8, 16, 128)
        values[:, at, :] = both[:, 128:].astype(BF16).reshape(8, 16, 128)
        gates[at, :] = pre
        score(src, key_rows)

    def made(q, which):
        dz, dy = MADE[q]
        at = positions(here)
        src, dst = (
            (made_keys.at[q], keys.at[:, at, :]),
            (made_values.at[q], values.at[:, at, :]),
            (made_gates.at[q], gates.at[at, :]),
        )[which]
        return pltpu.make_async_remote_copy(
            src_ref=src,
            dst_ref=dst,
            send_sem=made_send.at[q, which],
            recv_sem=made_recv.at[q, which],
            device_id={"z": zs[dz], "y": ys[dy]},
            device_id_type=MESH,
        )

    def make(q):
        both, pre = products(made_rows[q].reshape(128, 1024))
        made_keys[q] = both[:, :128].astype(BF16).reshape(8, 16, 128)
        made_values[q] = both[:, 128:].astype(BF16).reshape(8, 16, 128)
        made_gates[q] = pre

    def send_made(q):
        for which in range(3):
            made(q, which).start()

    def finish_made(q):
        for which in range(3):
            made(q, which).wait_recv()
        src = zs[-MADE[q][0]] * 4 + ys[-MADE[q][1]]
        score(src, keys[:, positions(src), :].reshape(128, 128))

    project(here)
    pl.semaphore_wait(line_in, 3)
    for k in range(1, 5):
        far(k).start()

    def arrive(k):
        far(k).wait_recv()
        along_x(k, 0).start()
        along_x(k, 1).start()
        if k >= DIRECT:
            along_x(k, 2).start()
        if k + 5 < FAR:
            far(k + 5).start()

    def relay(k):
        along_x(k, 0).wait_recv()
        along_x(k, 2).start()

    def start_swap(k):
        if k >= DIRECT:
            along_x(k, 0).wait_recv()
        along_x(k, 1).wait_recv()
        along_x(k, 2).wait_recv()
        swap(k, source(k)).start()

    def finish(k):
        swap(k, source(k)).wait_recv()
        project(source(k))

    def start_near(k):
        near(k).start()

    def swap_near(k):
        near(k).wait_recv()
        swap(FAR + k, near_source(k)).start()

    def finish_near(k):
        swap(FAR + k, near_source(k)).wait_recv()
        project(near_source(k))

    events = []
    for k in range(FAR):
        events.append((k, 0, arrive, k))
        if k < DIRECT:
            events.append((k + 3, 2, relay, k))
        events.append((k + 7, 3, start_swap, k))
        events.append((k + 9, 4, finish, k))
    for k in range(3):
        if (0, 0, 0)[k]:
            events.append(((0, 0, 0)[k], 5, start_near, k))
        events.append(((6, 7, 8)[k], 6, swap_near, k))
        events.append(((9, 10, 11)[k], 7, finish_near, k))
    for q in range(len(MADE)):
        events.append(((-1, 0, 1, 2)[q], 7, make, q))
        events.append(((5, 5, 6, 7)[q], 8, send_made, q))
        events.append(((12, 13, 14, 15)[q], 9, finish_made, q))
    for _, _, stage, k in sorted(events, key=lambda e: (e[0], e[1], e[3])):
        stage(k)

    lane1 = lax.broadcasted_iota(jnp.int32, (1, 128), 1)
    bias = jnp.where(
        lane1 < 16,
        jnp.where(lane1 < 8, biases[0:1, 0:1], biases[0:1, 1:2]),
        jnp.where(lane1 < 24, biases[1:2, 0:1], biases[1:2, 1:2]),
    )
    pre = gates[...] + bias
    forget = pltpu.roll(jax.nn.log_sigmoid(pre), 112, 1)
    row = lax.broadcasted_iota(jnp.int32, (256, 256), 0)
    col = lax.broadcasted_iota(jnp.int32, (256, 256), 1)
    lower = jnp.where(col < row, 1.0, 0.0)
    before = jnp.dot(lower, forget, preferred_element_type=F32, precision=lax.Precision.HIGHEST)
    total = before[255:256, :] + forget[255:256, :]
    log_weight = pre + jnp.where(lane1 < 8, total - before - forget, before)
    stable = jnp.maximum(total, jnp.max(log_weight, axis=0, keepdims=True))
    weight = jnp.exp(log_weight - stable) * 128.0**-0.5
    stable_out[0:1, :] = stable[:, 0:8]
    stable_out[1:2, :] = pltpu.roll(stable, 120, 1)[:, 0:8]

    read_weight = weight * scores[...]
    denominator = jnp.sum(read_weight, axis=0, keepdims=True)
    floor_value = jnp.maximum(jnp.maximum(jnp.abs(denominator), jnp.exp(-stable)), 1.0)
    read_weight = read_weight / floor_value
    read_weight = read_weight + pltpu.roll(read_weight, 120, 1)
    by_seq = read_weight.T[0:8]
    high = by_seq.astype(BF16)
    both_parts = jnp.concatenate([high.astype(F32), by_seq - high.astype(F32)], axis=0).astype(BF16)
    hidden = []
    for b in range(8):
        two = jnp.dot(both_parts, values[b], preferred_element_type=F32)
        hidden.append(two[b : b + 1] + two[8 + b : 9 + b])
    hidden = jnp.concatenate(hidden, axis=0).astype(BF16)
    head_terms = jnp.dot(hidden, out_w[...], preferred_element_type=F32)
    for t in range(8):
        terms[t] = head_terms[:, 128 * t : 128 * t + 128]

    me = 2 * x + c

    def term(k):
        tx, tc = xs[k // 2], cs[k % 2]
        return pltpu.make_async_remote_copy(
            src_ref=terms.at[2 * tx + tc],
            dst_ref=parts.at[k],
            send_sem=term_send.at[k],
            recv_sem=term_recv.at[k],
            device_id={"x": tx, "c": tc},
            device_id_type=MESH,
        )

    for k in range(1, 8):
        term(k).start()

    for b in range(8):
        float_keys = keys[b].astype(F32)
        float_values = values[b].astype(F32)
        weighted = []
        for g in range(2):
            spread_weight = jnp.broadcast_to(weight[:, 8 * g + b : 8 * g + b + 1], (256, 128))
            weighted.append((float_values * spread_weight).astype(BF16))
            normal_out[g, b : b + 1, :] = jnp.sum(float_keys * spread_weight, axis=0, keepdims=True)
        cells = lax.dot_general(
            keys[b], jnp.concatenate(weighted, axis=1), (((0,), (0,)), ((), ())), preferred_element_type=F32
        ).astype(BF16)
        memory_out[0, b] = cells[:, :128]
        memory_out[1, b] = cells[:, 128:]

    for k in range(FAR):
        far(k).wait_send()
        swap(k, source(k)).wait_send()
        for which in range(3):
            along_x(k, which).wait_send()

    for q in range(len(MADE)):
        for which in range(3):
            made(q, which).wait_send()
    for k in range(3):
        near(k).wait_send()
        swap(FAR + k, near_source(k)).wait_send()

    for k in range(1, 8):
        term(k).wait_recv()

    total_read = terms[me]
    for k in range(1, 8):
        total_read = total_read + parts[k]
    read_out[...] = total_read.astype(BF16)

    for k in range(1, 8):
        term(k).wait_send()


def write_out(memory, normal, stable, read, memory_out, normal_out, stable_out, read_out, sems):
    pairs = ((memory, memory_out), (normal, normal_out), (stable, stable_out), (read, read_out))
    copies = [pltpu.make_async_copy(a, b, sems.at[k]) for k, (a, b) in enumerate(pairs)]
    for copy in copies:
        copy.start()
    for copy in copies:
        copy.wait()


def shards(prompt, w_key, w_value, w_in_gate, w_forget_gate, in_bias, forget_bias, query, w_out):
    vmem = pl.BlockSpec(memory_space=pltpu.VMEM)
    hbm = pl.BlockSpec(memory_space=pltpu.HBM)
    dma = pltpu.SemaphoreType.DMA
    memory, normal, stable, read = pl.pallas_call(
        kernel,
        out_shape=(
            jax.ShapeDtypeStruct((2, 8, 128, 128), BF16),
            jax.ShapeDtypeStruct((2, 8, 128), F32),
            jax.ShapeDtypeStruct((2, 8), F32),
            jax.ShapeDtypeStruct((8, 128), BF16),
        ),
        in_specs=[hbm] * 9,
        out_specs=(vmem, vmem, vmem, vmem),
        scratch_shapes=[
            pltpu.VMEM((16, 8, 16, 1024), BF16),
            pltpu.VMEM((1024, 256), BF16),
            pltpu.VMEM((2, 2, 1024), BF16),
            pltpu.VMEM((1024, 128), BF16),
            pltpu.VMEM((2, 2), F32),
            pltpu.VMEM((8, 128), BF16),
            pltpu.VMEM((128, 128), BF16),
            pltpu.VMEM((128, 1024), BF16),
            pltpu.VMEM((8, 256, 128), BF16),
            pltpu.VMEM((8, 256, 128), BF16),
            pltpu.VMEM((256, 128), F32),
            pltpu.VMEM((256, 128), F32),
            pltpu.VMEM((4, 8, 16, 1024), BF16),
            pltpu.VMEM((4, 8, 16, 128), BF16),
            pltpu.VMEM((4, 8, 16, 128), BF16),
            pltpu.VMEM((4, 16, 128), F32),
            pltpu.VMEM((8, 8, 128), F32),
            pltpu.VMEM((8, 8, 128), F32),
            dma((13,)),
            dma((FAR,)),
            dma((FAR,)),
            pltpu.SemaphoreType.REGULAR,
            dma((4, 3)),
            dma((4, 3)),
            dma((3,)),
            dma((3,)),
            dma((FAR, 3)),
            dma((FAR, 3)),
            dma((FAR + 3,)),
            dma((FAR + 3,)),
            dma((8,)),
            dma((8,)),
        ],
        compiler_params=pltpu.CompilerParams(
            collective_id=0, has_side_effects=True, vmem_limit_bytes=20 * 1024 * 1024
        ),
    )(
        *(pltpu.with_memory_space_constraint(v, pltpu.HBM) for v in (
            prompt, w_key[:, 0], w_value[:, 0], w_in_gate[:, :, 0], w_forget_gate[:, :, 0],
            in_bias.T, forget_bias.T, query[:, 0], w_out[0],
        ))
    )
    memory, normal, stable, read = pl.pallas_call(
        write_out,
        out_shape=tuple(jax.ShapeDtypeStruct(v.shape, v.dtype) for v in (memory, normal, stable, read)),
        in_specs=[vmem] * 4,
        out_specs=(hbm,) * 4,
        scratch_shapes=[dma((4,))],
        compiler_params=pltpu.CompilerParams(vmem_limit_bytes=4 * 1024 * 1024),
    )(memory, normal, stable, read)
    return memory[:, :, None], normal[:, :, None], stable[:, :, None], read


def solution(mesh):
    torus = Mesh(
        mesh.devices.reshape(mesh.shape["gr"], 4, 4, 4, 2), ("gr", "z", "y", "x", "c")
    )
    sp = ("z", "y")
    both = ("gr", "z", "y")
    return jax.shard_map(
        shards,
        mesh=torus,
        in_specs=(
            P("gr", sp, None),
            P(None, TP, None),
            P(None, TP, None),
            P(None, None, TP),
            P(None, None, TP),
            P(None, TP),
            P(None, TP),
            P(both, TP, None),
            P(TP, None, None),
        ),
        out_specs=(
            P(None, both, TP, None, None),
            P(None, both, TP, None),
            P(None, both, TP),
            P(both, TP),
        ),
        check_vma=False,
    )
```

```python
import functools

import jax
import jax.numpy as jnp
from jax import lax
from jax.experimental import pallas as pl
from jax.experimental.pallas import tpu as pltpu
from jax.sharding import Mesh
from jax.sharding import PartitionSpec as P

MESH = pl.DeviceIdType.MESH
TP = ("x", "c")
F32 = jnp.float32
BF16 = jnp.bfloat16
FAR = 8


OFFSETS = [(2, 0), (2, 1), (3, 1), (1, 3), (2, 3), (1, 2), (2, 2), (3, 2)]
MADE = [(1, 0), (3, 0), (1, 1), (3, 3)]
DIRECT = FAR - 8
NEAR = (1, 3, 2)


def kernel(
    prompt, w_key, w_value, w_in, w_forget, in_bias, forget_bias, query, w_out,
    memory_out, normal_out, stable_out, read_out,
    rows, weights, gate_rows, gate_w, biases, queries, query_w, out_w, keys, values, gates, scores, made_rows, made_keys, made_values, made_gates, terms, parts,
    load_sem, far_send, far_recv, line_in, made_send, made_recv, near_send, near_recv, x_send, x_recv, swap_send, swap_recv, term_send, term_recv,
):
    z, y, x, c = (lax.axis_index(a) for a in ("z", "y", "x", "c"))
    here = z * 4 + y
    zs = [z] + [lax.rem(z + k, 4) for k in range(1, 4)]
    ys = [y] + [lax.rem(y + k, 4) for k in range(1, 4)]
    xs = [x] + [lax.rem(x + k, 4) for k in range(1, 4)]
    cs = [c, 1 - c]
    seq = 4 * c + x
    up = lax.rem(x + 1 + 2 * c, 4)
    down = lax.rem(x + 3 + 2 * c, 4)

    loads = [
        pltpu.make_async_copy(w_key, weights.at[:, pl.ds(0, 128)], load_sem.at[0]),
        pltpu.make_async_copy(w_value, weights.at[:, pl.ds(128, 128)], load_sem.at[1]),
        pltpu.make_async_copy(prompt.at[pl.ds(here * 8, 8)], rows.at[here], load_sem.at[2]),
        pltpu.make_async_copy(w_in, gate_rows.at[0], load_sem.at[3]),
        pltpu.make_async_copy(w_forget, gate_rows.at[1], load_sem.at[4]),
        pltpu.make_async_copy(in_bias, biases.at[pl.ds(0, 1)], load_sem.at[5]),
        pltpu.make_async_copy(forget_bias, biases.at[pl.ds(1, 1)], load_sem.at[6]),
        pltpu.make_async_copy(query, queries, load_sem.at[7]),
        pltpu.make_async_copy(w_out, out_w, load_sem.at[8]),
    ]
    for q, (dz, dy) in enumerate(MADE):
        there = (zs[dz] * 4 + ys[dy]) * 8
        loads.append(pltpu.make_async_copy(prompt.at[pl.ds(there, 8)], made_rows.at[q], load_sem.at[9 + q]))
    for load in loads:
        load.start()

    barrier = pltpu.get_barrier_semaphore()

    for k in range(3, 0, -1):
        pl.semaphore_signal(barrier, inc=1, device_id={"z": zs[k]}, device_id_type=MESH)
        pl.semaphore_signal(barrier, inc=1, device_id={"y": ys[k]}, device_id_type=MESH)
    for k in range(7, 0, -1):
        to = {"x": xs[k // 2], "c": cs[k % 2]}
        pl.semaphore_signal(barrier, inc=1, device_id=to, device_id_type=MESH)

    pl.semaphore_wait(barrier, 13)

    def far(k):
        dz, dy = OFFSETS[k]
        tz, ty = zs[dz], ys[dy]
        return pltpu.make_async_remote_copy(
            src_ref=prompt.at[(tz * 4 + ty) * 8 + seq],
            dst_ref=rows.at[here, seq],
            send_sem=far_send.at[k],
            recv_sem=far_recv.at[k],
            device_id={"z": tz, "y": ty},
            device_id_type=MESH,
        )

    def near(k):
        ty = ys[NEAR[k]]
        return pltpu.make_async_remote_copy(
            src_ref=prompt.at[pl.ds((z * 4 + ty) * 8 + 4 * c, 4)],
            dst_ref=rows.at[here, pl.ds(4 * c, 4)],
            send_sem=near_send.at[k],
            recv_sem=near_recv.at[k],
            device_id={"y": ty},
            device_id_type=MESH,
        )

    def source(k):
        dz, dy = OFFSETS[k]
        return zs[-dz] * 4 + ys[-dy]

    def near_source(k):
        return z * 4 + ys[4 - NEAR[k]]

    def along_x(k, which):
        direct = k >= DIRECT
        block = rows.at[source(k), seq if which < 2 or direct else 4 * c + down]
        return pltpu.make_async_remote_copy(
            src_ref=block,
            dst_ref=block,
            send_sem=x_send.at[k, which],
            recv_sem=x_recv.at[k, which],
            device_id={"x": (up, down, xs[2] if direct else up)[which]},
            device_id_type=MESH,
        )

    def swap(k, src):
        block = rows.at[src, pl.ds(4 * c, 4)]
        return pltpu.make_async_remote_copy(
            src_ref=block,
            dst_ref=block,
            send_sem=swap_send.at[k],
            recv_sem=swap_recv.at[k],
            device_id={"c": cs[1]},
            device_id_type=MESH,
        )

    for k in range(3, 0, -1):
        pl.semaphore_signal(line_in, inc=1, device_id={"y": ys[k]}, device_id_type=MESH)
    for k in range(1):
        far(k).start()
    near(0).start()
    near(1).start()
    near(2).start()

    for load in loads:
        load.wait()

    lane_gate = lax.broadcasted_iota(jnp.int32, (2, 128), 1) // 8
    gate2 = lax.broadcasted_iota(jnp.int32, (2, 128), 0)
    spread_gates = 0.0
    for kind in range(2):
        spread = jnp.where(lane_gate == 2 * kind + gate2, 1.0, 0.0).astype(BF16)
        spread_gates = spread_gates + lax.dot_general(
            gate_rows[kind], spread, (((0,), (0,)), ((), ())), preferred_element_type=F32
        )
    gate_w[...] = spread_gates.astype(BF16)

    lane8 = lax.broadcasted_iota(jnp.int32, (8, 128), 1)
    pick = jnp.where(lax.rem(lane8, 8) == lax.broadcasted_iota(jnp.int32, (8, 128), 0), 1.0, 0.0)
    query_w[...] = lax.dot_general(
        queries[...], pick.astype(BF16), (((0,), (0,)), ((), ())), preferred_element_type=F32
    ).astype(BF16)

    lane = lax.broadcasted_iota(jnp.int32, (8, 16, 128), 2)
    which_seq = lax.broadcasted_iota(jnp.int32, (8, 16, 128), 0)
    own_lane = lax.rem(lane, 8) == which_seq

    def products(block):
        both = jnp.dot(block, weights[...], preferred_element_type=F32)
        pre = jnp.dot(block, gate_w[...], preferred_element_type=F32).reshape(8, 16, 128)
        return both, jnp.sum(jnp.where(own_lane, pre, 0.0), axis=0)

    def positions(src):
        return pl.ds(pl.multiple_of(src * 16, 16), 16)

    def score(src, key_rows):
        every = jnp.dot(key_rows, query_w[...], preferred_element_type=F32).reshape(8, 16, 128)
        scores[positions(src), :] = jnp.sum(jnp.where(own_lane, every, 0.0), axis=0)

    def project(src):
        both, pre = products(rows[src].reshape(128, 1024))
        at = positions(src)
        key_rows = both[:, :128].astype(BF16)
        keys[:, at, :] = key_rows.reshape(8, 16, 128)
        values[:, at, :] = both[:, 128:].astype(BF16).reshape(8, 16, 128)
        gates[at, :] = pre
        score(src, key_rows)

    def made(q, which):
        dz, dy = MADE[q]
        at = positions(here)
        src, dst = (
            (made_keys.at[q], keys.at[:, at, :]),
            (made_values.at[q], values.at[:, at, :]),
            (made_gates.at[q], gates.at[at, :]),
        )[which]
        return pltpu.make_async_remote_copy(
            src_ref=src,
            dst_ref=dst,
            send_sem=made_send.at[q, which],
            recv_sem=made_recv.at[q, which],
            device_id={"z": zs[dz], "y": ys[dy]},
            device_id_type=MESH,
        )

    def make(q):
        both, pre = products(made_rows[q].reshape(128, 1024))
        made_keys[q] = both[:, :128].astype(BF16).reshape(8, 16, 128)
        made_values[q] = both[:, 128:].astype(BF16).reshape(8, 16, 128)
        made_gates[q] = pre

    def send_made(q):
        for which in range(3):
            made(q, which).start()

    def finish_made(q):
        for which in range(3):
            made(q, which).wait_recv()
        src = zs[-MADE[q][0]] * 4 + ys[-MADE[q][1]]
        score(src, keys[:, positions(src), :].reshape(128, 128))

    project(here)
    pl.semaphore_wait(line_in, 3)
    for k in range(1, 5):
        far(k).start()

    def arrive(k):
        far(k).wait_recv()
        along_x(k, 0).start()
        along_x(k, 1).start()
        if k >= DIRECT:
            along_x(k, 2).start()
        if k + 5 < FAR:
            far(k + 5).start()

    def relay(k):
        along_x(k, 0).wait_recv()
        along_x(k, 2).start()

    def start_swap(k):
        if k >= DIRECT:
            along_x(k, 0).wait_recv()
        along_x(k, 1).wait_recv()
        along_x(k, 2).wait_recv()
        swap(k, source(k)).start()

    def finish(k):
        swap(k, source(k)).wait_recv()
        project(source(k))

    def start_near(k):
        near(k).start()

    def swap_near(k):
        near(k).wait_recv()
        swap(FAR + k, near_source(k)).start()

    def finish_near(k):
        swap(FAR + k, near_source(k)).wait_recv()
        project(near_source(k))

    events = []
    for k in range(FAR):
        events.append((k, 0, arrive, k))
        if k < DIRECT:
            events.append((k + 3, 2, relay, k))
        events.append((k + 7, 3, start_swap, k))
        events.append((k + 9, 4, finish, k))
    for k in range(3):
        if (0, 0, 0)[k]:
            events.append(((0, 0, 0)[k], 5, start_near, k))
        events.append(((4, 5, 6)[k], 6, swap_near, k))
        events.append(((6, 7, 8)[k], 7, finish_near, k))
    for q in range(len(MADE)):
        events.append(((-1, 0, 1, 2)[q], 7, make, q))
        events.append(((5, 5, 6, 7)[q], 8, send_made, q))
        events.append(((12, 13, 14, 15)[q], 9, finish_made, q))
    for _, _, stage, k in sorted(events, key=lambda e: (e[0], e[1], e[3])):
        stage(k)

    lane1 = lax.broadcasted_iota(jnp.int32, (1, 128), 1)
    bias = jnp.where(
        lane1 < 16,
        jnp.where(lane1 < 8, biases[0:1, 0:1], biases[0:1, 1:2]),
        jnp.where(lane1 < 24, biases[1:2, 0:1], biases[1:2, 1:2]),
    )
    pre = gates[...] + bias
    forget = pltpu.roll(jax.nn.log_sigmoid(pre), 112, 1)
    row = lax.broadcasted_iota(jnp.int32, (256, 256), 0)
    col = lax.broadcasted_iota(jnp.int32, (256, 256), 1)
    lower = jnp.where(col < row, 1.0, 0.0).astype(BF16)
    high = forget.astype(BF16).astype(F32)
    middle = (forget - high).astype(BF16).astype(F32)
    low = forget - high - middle
    split = jnp.where(
        lane1 < 16, high, jnp.where(lane1 < 32, pltpu.roll(middle, 16, 1), jnp.where(lane1 < 48, pltpu.roll(low, 32, 1), 0.0))
    )
    sums = jnp.dot(lower, split.astype(BF16), preferred_element_type=F32)
    before = sums + pltpu.roll(sums, 112, 1) + pltpu.roll(sums, 96, 1)
    total = before[255:256, :] + forget[255:256, :]
    log_weight = pre + jnp.where(lane1 < 8, total - before - forget, before)
    stable = jnp.maximum(total, jnp.max(log_weight, axis=0, keepdims=True))
    weight = jnp.exp(log_weight - stable) * 128.0**-0.5
    stable_out[0:1, :] = stable[:, 0:8]
    stable_out[1:2, :] = pltpu.roll(stable, 120, 1)[:, 0:8]

    read_weight = weight * scores[...]
    denominator = jnp.sum(read_weight, axis=0, keepdims=True)
    floor_value = jnp.maximum(jnp.maximum(jnp.abs(denominator), jnp.exp(-stable)), 1.0)
    read_weight = read_weight / floor_value
    read_weight = read_weight + pltpu.roll(read_weight, 120, 1)
    by_seq = read_weight.T[0:8]
    high = by_seq.astype(BF16)
    both_parts = jnp.concatenate([high.astype(F32), by_seq - high.astype(F32)], axis=0).astype(BF16)
    hidden = []
    for b in range(8):
        two = jnp.dot(both_parts, values[b], preferred_element_type=F32)
        hidden.append(two[b : b + 1] + two[8 + b : 9 + b])
    hidden = jnp.concatenate(hidden, axis=0).astype(BF16)
    head_terms = jnp.dot(hidden, out_w[...], preferred_element_type=F32)
    for t in range(8):
        terms[t] = head_terms[:, 128 * t : 128 * t + 128]

    me = 2 * x + c

    def term(k):
        tx, tc = xs[k // 2], cs[k % 2]
        return pltpu.make_async_remote_copy(
            src_ref=terms.at[2 * tx + tc],
            dst_ref=parts.at[k],
            send_sem=term_send.at[k],
            recv_sem=term_recv.at[k],
            device_id={"x": tx, "c": tc},
            device_id_type=MESH,
        )

    for k in range(1, 8):
        term(k).start()

    for b in range(8):
        float_keys = keys[b].astype(F32)
        float_values = values[b].astype(F32)
        weighted = []
        for g in range(2):
            spread_weight = jnp.broadcast_to(weight[:, 8 * g + b : 8 * g + b + 1], (256, 128))
            weighted.append((float_values * spread_weight).astype(BF16))
            normal_out[g, b : b + 1, :] = jnp.sum(float_keys * spread_weight, axis=0, keepdims=True)
        cells = lax.dot_general(
            keys[b], jnp.concatenate(weighted, axis=1), (((0,), (0,)), ((), ())), preferred_element_type=F32
        ).astype(BF16)
        memory_out[0, b] = cells[:, :128]
        memory_out[1, b] = cells[:, 128:]

    for k in range(FAR):
        far(k).wait_send()
        swap(k, source(k)).wait_send()
        for which in range(3):
            along_x(k, which).wait_send()

    for q in range(len(MADE)):
        for which in range(3):
            made(q, which).wait_send()
    for k in range(3):
        near(k).wait_send()
        swap(FAR + k, near_source(k)).wait_send()

    for k in range(1, 8):
        term(k).wait_recv()

    total_read = terms[me]
    for k in range(1, 8):
        total_read = total_read + parts[k]
    read_out[...] = total_read.astype(BF16)

    for k in range(1, 8):
        term(k).wait_send()


def write_out(memory, normal, stable, read, memory_out, normal_out, stable_out, read_out, sems):
    pairs = ((memory, memory_out), (normal, normal_out), (stable, stable_out), (read, read_out))
    copies = [pltpu.make_async_copy(a, b, sems.at[k]) for k, (a, b) in enumerate(pairs)]
    for copy in copies:
        copy.start()
    for copy in copies:
        copy.wait()


def shards(prompt, w_key, w_value, w_in_gate, w_forget_gate, in_bias, forget_bias, query, w_out):
    vmem = pl.BlockSpec(memory_space=pltpu.VMEM)
    hbm = pl.BlockSpec(memory_space=pltpu.HBM)
    dma = pltpu.SemaphoreType.DMA
    memory, normal, stable, read = pl.pallas_call(
        kernel,
        out_shape=(
            jax.ShapeDtypeStruct((2, 8, 128, 128), BF16),
            jax.ShapeDtypeStruct((2, 8, 128), F32),
            jax.ShapeDtypeStruct((2, 8), F32),
            jax.ShapeDtypeStruct((8, 128), BF16),
        ),
        in_specs=[hbm] * 9,
        out_specs=(vmem, vmem, vmem, vmem),
        scratch_shapes=[
            pltpu.VMEM((16, 8, 16, 1024), BF16),
            pltpu.VMEM((1024, 256), BF16),
            pltpu.VMEM((2, 2, 1024), BF16),
            pltpu.VMEM((1024, 128), BF16),
            pltpu.VMEM((2, 2), F32),
            pltpu.VMEM((8, 128), BF16),
            pltpu.VMEM((128, 128), BF16),
            pltpu.VMEM((128, 1024), BF16),
            pltpu.VMEM((8, 256, 128), BF16),
            pltpu.VMEM((8, 256, 128), BF16),
            pltpu.VMEM((256, 128), F32),
            pltpu.VMEM((256, 128), F32),
            pltpu.VMEM((4, 8, 16, 1024), BF16),
            pltpu.VMEM((4, 8, 16, 128), BF16),
            pltpu.VMEM((4, 8, 16, 128), BF16),
            pltpu.VMEM((4, 16, 128), F32),
            pltpu.VMEM((8, 8, 128), F32),
            pltpu.VMEM((8, 8, 128), F32),
            dma((13,)),
            dma((FAR,)),
            dma((FAR,)),
            pltpu.SemaphoreType.REGULAR,
            dma((4, 3)),
            dma((4, 3)),
            dma((3,)),
            dma((3,)),
            dma((FAR, 3)),
            dma((FAR, 3)),
            dma((FAR + 3,)),
            dma((FAR + 3,)),
            dma((8,)),
            dma((8,)),
        ],
        compiler_params=pltpu.CompilerParams(
            collective_id=0, has_side_effects=True, vmem_limit_bytes=20 * 1024 * 1024
        ),
    )(
        *(pltpu.with_memory_space_constraint(v, pltpu.HBM) for v in (
            prompt, w_key[:, 0], w_value[:, 0], w_in_gate[:, :, 0], w_forget_gate[:, :, 0],
            in_bias.T, forget_bias.T, query[:, 0], w_out[0],
        ))
    )
    memory, normal, stable, read = pl.pallas_call(
        write_out,
        out_shape=tuple(jax.ShapeDtypeStruct(v.shape, v.dtype) for v in (memory, normal, stable, read)),
        in_specs=[vmem] * 4,
        out_specs=(hbm,) * 4,
        scratch_shapes=[dma((4,))],
        compiler_params=pltpu.CompilerParams(vmem_limit_bytes=4 * 1024 * 1024),
    )(memory, normal, stable, read)
    return memory[:, :, None], normal[:, :, None], stable[:, :, None], read


def solution(mesh):
    torus = Mesh(
        mesh.devices.reshape(mesh.shape["gr"], 4, 4, 4, 2), ("gr", "z", "y", "x", "c")
    )
    sp = ("z", "y")
    both = ("gr", "z", "y")
    return jax.shard_map(
        shards,
        mesh=torus,
        in_specs=(
            P("gr", sp, None),
            P(None, TP, None),
            P(None, TP, None),
            P(None, None, TP),
            P(None, None, TP),
            P(None, TP),
            P(None, TP),
            P(both, TP, None),
            P(TP, None, None),
        ),
        out_specs=(
            P(None, both, TP, None, None),
            P(None, both, TP, None),
            P(None, both, TP),
            P(both, TP),
        ),
        check_vma=False,
    )
```

```python
import functools

import jax
import jax.numpy as jnp
from jax import lax
from jax.experimental import pallas as pl
from jax.experimental.pallas import tpu as pltpu
from jax.sharding import Mesh
from jax.sharding import PartitionSpec as P

MESH = pl.DeviceIdType.MESH
TP = ("x", "c")
F32 = jnp.float32
BF16 = jnp.bfloat16
FAR = 8


OFFSETS = [(2, 0), (2, 1), (3, 1), (1, 3), (2, 3), (1, 2), (2, 2), (3, 2)]
MADE = [(1, 0), (3, 0), (1, 1), (3, 3)]
DIRECT = FAR - 8
NEAR = (1, 3, 2)


def kernel(
    prompt, w_key, w_value, w_in, w_forget, in_bias, forget_bias, query, w_out,
    memory_out, normal_out, stable_out, read_out,
    rows, weights, gate_rows, gate_w, biases, queries, query_w, out_w, keys, values, gates, scores, made_rows, made_keys, made_values, made_gates, terms, parts,
    load_sem, far_send, far_recv, line_in, made_send, made_recv, near_send, near_recv, x_send, x_recv, swap_send, swap_recv, term_send, term_recv,
):
    z, y, x, c = (lax.axis_index(a) for a in ("z", "y", "x", "c"))
    here = z * 4 + y
    zs = [z] + [lax.rem(z + k, 4) for k in range(1, 4)]
    ys = [y] + [lax.rem(y + k, 4) for k in range(1, 4)]
    xs = [x] + [lax.rem(x + k, 4) for k in range(1, 4)]
    cs = [c, 1 - c]
    seq = 4 * c + x
    up = lax.rem(x + 1 + 2 * c, 4)
    down = lax.rem(x + 3 + 2 * c, 4)

    loads = [
        pltpu.make_async_copy(w_key, weights.at[:, pl.ds(0, 128)], load_sem.at[0]),
        pltpu.make_async_copy(w_value, weights.at[:, pl.ds(128, 128)], load_sem.at[1]),
        pltpu.make_async_copy(prompt.at[pl.ds(here * 8, 8)], rows.at[here], load_sem.at[2]),
        pltpu.make_async_copy(w_in, gate_rows.at[0], load_sem.at[3]),
        pltpu.make_async_copy(w_forget, gate_rows.at[1], load_sem.at[4]),
        pltpu.make_async_copy(in_bias, biases.at[pl.ds(0, 1)], load_sem.at[5]),
        pltpu.make_async_copy(forget_bias, biases.at[pl.ds(1, 1)], load_sem.at[6]),
        pltpu.make_async_copy(query, queries, load_sem.at[7]),
        pltpu.make_async_copy(w_out, out_w, load_sem.at[8]),
    ]
    for q, (dz, dy) in enumerate(MADE):
        there = (zs[dz] * 4 + ys[dy]) * 8
        loads.append(pltpu.make_async_copy(prompt.at[pl.ds(there, 8)], made_rows.at[q], load_sem.at[9 + q]))
    barrier = pltpu.get_barrier_semaphore()

    for k in range(3, 0, -1):
        pl.semaphore_signal(barrier, inc=1, device_id={"z": zs[k]}, device_id_type=MESH)
        pl.semaphore_signal(barrier, inc=1, device_id={"y": ys[k]}, device_id_type=MESH)
    for k in range(7, 0, -1):
        to = {"x": xs[k // 2], "c": cs[k % 2]}
        pl.semaphore_signal(barrier, inc=1, device_id=to, device_id_type=MESH)

    for load in loads:
        load.start()
    pl.semaphore_wait(barrier, 13)

    def far(k):
        dz, dy = OFFSETS[k]
        tz, ty = zs[dz], ys[dy]
        return pltpu.make_async_remote_copy(
            src_ref=prompt.at[(tz * 4 + ty) * 8 + seq],
            dst_ref=rows.at[here, seq],
            send_sem=far_send.at[k],
            recv_sem=far_recv.at[k],
            device_id={"z": tz, "y": ty},
            device_id_type=MESH,
        )

    def near(k):
        ty = ys[NEAR[k]]
        return pltpu.make_async_remote_copy(
            src_ref=prompt.at[pl.ds((z * 4 + ty) * 8 + 4 * c, 4)],
            dst_ref=rows.at[here, pl.ds(4 * c, 4)],
            send_sem=near_send.at[k],
            recv_sem=near_recv.at[k],
            device_id={"y": ty},
            device_id_type=MESH,
        )

    def source(k):
        dz, dy = OFFSETS[k]
        return zs[-dz] * 4 + ys[-dy]

    def near_source(k):
        return z * 4 + ys[4 - NEAR[k]]

    def along_x(k, which):
        direct = k >= DIRECT
        block = rows.at[source(k), seq if which < 2 or direct else 4 * c + down]
        return pltpu.make_async_remote_copy(
            src_ref=block,
            dst_ref=block,
            send_sem=x_send.at[k, which],
            recv_sem=x_recv.at[k, which],
            device_id={"x": (up, down, xs[2] if direct else up)[which]},
            device_id_type=MESH,
        )

    def swap(k, src):
        block = rows.at[src, pl.ds(4 * c, 4)]
        return pltpu.make_async_remote_copy(
            src_ref=block,
            dst_ref=block,
            send_sem=swap_send.at[k],
            recv_sem=swap_recv.at[k],
            device_id={"c": cs[1]},
            device_id_type=MESH,
        )

    for k in range(3, 0, -1):
        pl.semaphore_signal(line_in, inc=1, device_id={"y": ys[k]}, device_id_type=MESH)
    for k in range(1):
        far(k).start()
    near(0).start()
    near(1).start()
    near(2).start()

    for load in loads:
        load.wait()

    lane_gate = lax.broadcasted_iota(jnp.int32, (2, 128), 1) // 8
    gate2 = lax.broadcasted_iota(jnp.int32, (2, 128), 0)
    spread_gates = 0.0
    for kind in range(2):
        spread = jnp.where(lane_gate == 2 * kind + gate2, 1.0, 0.0).astype(BF16)
        spread_gates = spread_gates + lax.dot_general(
            gate_rows[kind], spread, (((0,), (0,)), ((), ())), preferred_element_type=F32
        )
    gate_w[...] = spread_gates.astype(BF16)

    lane8 = lax.broadcasted_iota(jnp.int32, (8, 128), 1)
    pick = jnp.where(lax.rem(lane8, 8) == lax.broadcasted_iota(jnp.int32, (8, 128), 0), 1.0, 0.0)
    query_w[...] = lax.dot_general(
        queries[...], pick.astype(BF16), (((0,), (0,)), ((), ())), preferred_element_type=F32
    ).astype(BF16)

    lane = lax.broadcasted_iota(jnp.int32, (8, 16, 128), 2)
    which_seq = lax.broadcasted_iota(jnp.int32, (8, 16, 128), 0)
    own_lane = lax.rem(lane, 8) == which_seq

    def products(block):
        both = jnp.dot(block, weights[...], preferred_element_type=F32)
        pre = jnp.dot(block, gate_w[...], preferred_element_type=F32).reshape(8, 16, 128)
        return both, jnp.sum(jnp.where(own_lane, pre, 0.0), axis=0)

    def positions(src):
        return pl.ds(pl.multiple_of(src * 16, 16), 16)

    def score(src, key_rows):
        every = jnp.dot(key_rows, query_w[...], preferred_element_type=F32).reshape(8, 16, 128)
        scores[positions(src), :] = jnp.sum(jnp.where(own_lane, every, 0.0), axis=0)

    def project(src):
        both, pre = products(rows[src].reshape(128, 1024))
        at = positions(src)
        key_rows = both[:, :128].astype(BF16)
        keys[:, at, :] = key_rows.reshape(8, 16, 128)
        values[:, at, :] = both[:, 128:].astype(BF16).reshape(8, 16, 128)
        gates[at, :] = pre
        score(src, key_rows)

    def made(q, which):
        dz, dy = MADE[q]
        at = positions(here)
        src, dst = (
            (made_keys.at[q], keys.at[:, at, :]),
            (made_values.at[q], values.at[:, at, :]),
            (made_gates.at[q], gates.at[at, :]),
        )[which]
        return pltpu.make_async_remote_copy(
            src_ref=src,
            dst_ref=dst,
            send_sem=made_send.at[q, which],
            recv_sem=made_recv.at[q, which],
            device_id={"z": zs[dz], "y": ys[dy]},
            device_id_type=MESH,
        )

    def make(q):
        both, pre = products(made_rows[q].reshape(128, 1024))
        made_keys[q] = both[:, :128].astype(BF16).reshape(8, 16, 128)
        made_values[q] = both[:, 128:].astype(BF16).reshape(8, 16, 128)
        made_gates[q] = pre

    def send_made(q):
        for which in range(3):
            made(q, which).start()

    def finish_made(q):
        for which in range(3):
            made(q, which).wait_recv()
        src = zs[-MADE[q][0]] * 4 + ys[-MADE[q][1]]
        score(src, keys[:, positions(src), :].reshape(128, 128))

    project(here)
    pl.semaphore_wait(line_in, 3)
    for k in range(1, 5):
        far(k).start()

    def arrive(k):
        far(k).wait_recv()
        along_x(k, 0).start()
        along_x(k, 1).start()
        if k >= DIRECT:
            along_x(k, 2).start()
        if k + 5 < FAR:
            far(k + 5).start()

    def relay(k):
        along_x(k, 0).wait_recv()
        along_x(k, 2).start()

    def start_swap(k):
        if k >= DIRECT:
            along_x(k, 0).wait_recv()
        along_x(k, 1).wait_recv()
        along_x(k, 2).wait_recv()
        swap(k, source(k)).start()

    def finish(k):
        swap(k, source(k)).wait_recv()
        project(source(k))

    def start_near(k):
        near(k).start()

    def swap_near(k):
        near(k).wait_recv()
        swap(FAR + k, near_source(k)).start()

    def finish_near(k):
        swap(FAR + k, near_source(k)).wait_recv()
        project(near_source(k))

    events = []
    for k in range(FAR):
        events.append((k, 0, arrive, k))
        if k < DIRECT:
            events.append((k + 3, 2, relay, k))
        events.append((k + 7, 3, start_swap, k))
        events.append((k + 9, 4, finish, k))
    for k in range(3):
        if (0, 0, 0)[k]:
            events.append(((0, 0, 0)[k], 5, start_near, k))
        events.append(((4, 5, 6)[k], 6, swap_near, k))
        events.append(((6, 7, 8)[k], 7, finish_near, k))
    for q in range(len(MADE)):
        events.append(((-1, 0, 1, 2)[q], 7, make, q))
        events.append(((5, 5, 6, 7)[q], 8, send_made, q))
        events.append(((12, 13, 14, 15)[q], 9, finish_made, q))
    for _, _, stage, k in sorted(events, key=lambda e: (e[0], e[1], e[3])):
        stage(k)

    lane1 = lax.broadcasted_iota(jnp.int32, (1, 128), 1)
    bias = jnp.where(
        lane1 < 16,
        jnp.where(lane1 < 8, biases[0:1, 0:1], biases[0:1, 1:2]),
        jnp.where(lane1 < 24, biases[1:2, 0:1], biases[1:2, 1:2]),
    )
    pre = gates[...] + bias
    forget = pltpu.roll(jax.nn.log_sigmoid(pre), 112, 1)
    row = lax.broadcasted_iota(jnp.int32, (256, 256), 0)
    col = lax.broadcasted_iota(jnp.int32, (256, 256), 1)
    lower = jnp.where(col < row, 1.0, 0.0).astype(BF16)
    high = forget.astype(BF16).astype(F32)
    middle = (forget - high).astype(BF16).astype(F32)
    low = forget - high - middle
    split = jnp.where(
        lane1 < 16, high, jnp.where(lane1 < 32, pltpu.roll(middle, 16, 1), jnp.where(lane1 < 48, pltpu.roll(low, 32, 1), 0.0))
    )
    sums = jnp.dot(lower, split.astype(BF16), preferred_element_type=F32)
    before = sums + pltpu.roll(sums, 112, 1) + pltpu.roll(sums, 96, 1)
    total = before[255:256, :] + forget[255:256, :]
    log_weight = pre + jnp.where(lane1 < 8, total - before - forget, before)
    stable = jnp.maximum(total, jnp.max(log_weight, axis=0, keepdims=True))
    weight = jnp.exp(log_weight - stable) * 128.0**-0.5
    stable_out[0:1, :] = stable[:, 0:8]
    stable_out[1:2, :] = pltpu.roll(stable, 120, 1)[:, 0:8]

    read_weight = weight * scores[...]
    denominator = jnp.sum(read_weight, axis=0, keepdims=True)
    floor_value = jnp.maximum(jnp.maximum(jnp.abs(denominator), jnp.exp(-stable)), 1.0)
    read_weight = read_weight / floor_value
    read_weight = read_weight + pltpu.roll(read_weight, 120, 1)
    by_seq = read_weight.T[0:8]
    high = by_seq.astype(BF16)
    both_parts = jnp.concatenate([high.astype(F32), by_seq - high.astype(F32)], axis=0).astype(BF16)
    hidden = []
    for b in range(8):
        two = jnp.dot(both_parts, values[b], preferred_element_type=F32)
        hidden.append(two[b : b + 1] + two[8 + b : 9 + b])
    hidden = jnp.concatenate(hidden, axis=0).astype(BF16)
    head_terms = jnp.dot(hidden, out_w[...], preferred_element_type=F32)
    for t in range(8):
        terms[t] = head_terms[:, 128 * t : 128 * t + 128]

    me = 2 * x + c

    def term(k):
        tx, tc = xs[k // 2], cs[k % 2]
        return pltpu.make_async_remote_copy(
            src_ref=terms.at[2 * tx + tc],
            dst_ref=parts.at[k],
            send_sem=term_send.at[k],
            recv_sem=term_recv.at[k],
            device_id={"x": tx, "c": tc},
            device_id_type=MESH,
        )

    for k in range(1, 8):
        term(k).start()

    for b in range(8):
        float_keys = keys[b].astype(F32)
        float_values = values[b].astype(F32)
        weighted = []
        for g in range(2):
            spread_weight = jnp.broadcast_to(weight[:, 8 * g + b : 8 * g + b + 1], (256, 128))
            weighted.append((float_values * spread_weight).astype(BF16))
            normal_out[g, b : b + 1, :] = jnp.sum(float_keys * spread_weight, axis=0, keepdims=True)
        cells = lax.dot_general(
            keys[b], jnp.concatenate(weighted, axis=1), (((0,), (0,)), ((), ())), preferred_element_type=F32
        ).astype(BF16)
        memory_out[0, b] = cells[:, :128]
        memory_out[1, b] = cells[:, 128:]

    for k in range(FAR):
        far(k).wait_send()
        swap(k, source(k)).wait_send()
        for which in range(3):
            along_x(k, which).wait_send()

    for q in range(len(MADE)):
        for which in range(3):
            made(q, which).wait_send()
    for k in range(3):
        near(k).wait_send()
        swap(FAR + k, near_source(k)).wait_send()

    for k in range(1, 8):
        term(k).wait_recv()

    total_read = terms[me]
    for k in range(1, 8):
        total_read = total_read + parts[k]
    read_out[...] = total_read.astype(BF16)

    for k in range(1, 8):
        term(k).wait_send()


def write_out(memory, normal, stable, read, memory_out, normal_out, stable_out, read_out, sems):
    pairs = ((memory, memory_out), (normal, normal_out), (stable, stable_out), (read, read_out))
    copies = [pltpu.make_async_copy(a, b, sems.at[k]) for k, (a, b) in enumerate(pairs)]
    for copy in copies:
        copy.start()
    for copy in copies:
        copy.wait()


def shards(prompt, w_key, w_value, w_in_gate, w_forget_gate, in_bias, forget_bias, query, w_out):
    vmem = pl.BlockSpec(memory_space=pltpu.VMEM)
    hbm = pl.BlockSpec(memory_space=pltpu.HBM)
    dma = pltpu.SemaphoreType.DMA
    memory, normal, stable, read = pl.pallas_call(
        kernel,
        out_shape=(
            jax.ShapeDtypeStruct((2, 8, 128, 128), BF16),
            jax.ShapeDtypeStruct((2, 8, 128), F32),
            jax.ShapeDtypeStruct((2, 8), F32),
            jax.ShapeDtypeStruct((8, 128), BF16),
        ),
        in_specs=[hbm] * 9,
        out_specs=(vmem, vmem, vmem, vmem),
        scratch_shapes=[
            pltpu.VMEM((16, 8, 16, 1024), BF16),
            pltpu.VMEM((1024, 256), BF16),
            pltpu.VMEM((2, 2, 1024), BF16),
            pltpu.VMEM((1024, 128), BF16),
            pltpu.VMEM((2, 2), F32),
            pltpu.VMEM((8, 128), BF16),
            pltpu.VMEM((128, 128), BF16),
            pltpu.VMEM((128, 1024), BF16),
            pltpu.VMEM((8, 256, 128), BF16),
            pltpu.VMEM((8, 256, 128), BF16),
            pltpu.VMEM((256, 128), F32),
            pltpu.VMEM((256, 128), F32),
            pltpu.VMEM((4, 8, 16, 1024), BF16),
            pltpu.VMEM((4, 8, 16, 128), BF16),
            pltpu.VMEM((4, 8, 16, 128), BF16),
            pltpu.VMEM((4, 16, 128), F32),
            pltpu.VMEM((8, 8, 128), F32),
            pltpu.VMEM((8, 8, 128), F32),
            dma((13,)),
            dma((FAR,)),
            dma((FAR,)),
            pltpu.SemaphoreType.REGULAR,
            dma((4, 3)),
            dma((4, 3)),
            dma((3,)),
            dma((3,)),
            dma((FAR, 3)),
            dma((FAR, 3)),
            dma((FAR + 3,)),
            dma((FAR + 3,)),
            dma((8,)),
            dma((8,)),
        ],
        compiler_params=pltpu.CompilerParams(
            collective_id=0, has_side_effects=True, vmem_limit_bytes=20 * 1024 * 1024
        ),
    )(
        *(pltpu.with_memory_space_constraint(v, pltpu.HBM) for v in (
            prompt, w_key[:, 0], w_value[:, 0], w_in_gate[:, :, 0], w_forget_gate[:, :, 0],
            in_bias.T, forget_bias.T, query[:, 0], w_out[0],
        ))
    )
    memory, normal, stable, read = pl.pallas_call(
        write_out,
        out_shape=tuple(jax.ShapeDtypeStruct(v.shape, v.dtype) for v in (memory, normal, stable, read)),
        in_specs=[vmem] * 4,
        out_specs=(hbm,) * 4,
        scratch_shapes=[dma((4,))],
        compiler_params=pltpu.CompilerParams(vmem_limit_bytes=4 * 1024 * 1024),
    )(memory, normal, stable, read)
    return memory[:, :, None], normal[:, :, None], stable[:, :, None], read


def solution(mesh):
    torus = Mesh(
        mesh.devices.reshape(mesh.shape["gr"], 4, 4, 4, 2), ("gr", "z", "y", "x", "c")
    )
    sp = ("z", "y")
    both = ("gr", "z", "y")
    return jax.shard_map(
        shards,
        mesh=torus,
        in_specs=(
            P("gr", sp, None),
            P(None, TP, None),
            P(None, TP, None),
            P(None, None, TP),
            P(None, None, TP),
            P(None, TP),
            P(None, TP),
            P(both, TP, None),
            P(TP, None, None),
        ),
        out_specs=(
            P(None, both, TP, None, None),
            P(None, both, TP, None),
            P(None, both, TP),
            P(both, TP),
        ),
        check_vma=False,
    )
```
